512 devices in a mesh: sp: 16 (over z), tp: 32 (over y, x, core).
Axes of the slice: x: 4, y: 4, z: 16, core: 2. Of those that a mesh axis runs over, the one named last changes fastest.
Arguments:
- latent: bfloat16 [6144, 2048], P('sp', 'tp'), may hold values from -12 to 12
- context: bfloat16 [512, 2048], P('sp', 'tp'), may hold values from -6 to 6
- cond: bfloat16 [2048], P('sp'), may hold values from -6 to 6
- cond_ctx: bfloat16 [2048], P('sp'), may hold values from -6 to 6
- w_mod: bfloat16 [2048, 3, 2048], P('sp', None, 'tp'), may hold values from -0.25 to 0.25
- g_norm: float32 [2048], P('tp'), may hold values from 0.1 to 1.9
- w_dq: bfloat16 [2048, 512], P('tp'), may hold values from -0.125 to 0.125
- w_dkv: bfloat16 [2048, 512], P('tp'), may hold values from -0.125 to 0.125
- w_kr: bfloat16 [2048, 64], P('tp'), may hold values from -0.125 to 0.125
- g_cq: float32 [512], replicated, may hold values from 0.5 to 32
- g_ckv: float32 [512], replicated, may hold values from 0.1 to 1.9
- w_uq: bfloat16 [512, 32, 192], P(None, 'tp'), may hold values from -0.25 to 0.25
- w_ukv: bfloat16 [512, 32, 256], P(None, 'tp'), may hold values from -0.25 to 0.25
- ctx_lift: float32 [32], P('tp'), may hold values from 1 to 3
- w_out: bfloat16 [32, 128, 2048], P('tp'), may hold values from -6 to 6
Outputs:
- mixed: bfloat16 [6144, 2048], P('sp', 'tp')
The draws below stay inside these ranges and needn't reach their ends.
All inputs are finite; a program needn't handle non-finite values.
Results may differ from the reference program's by a relative error of at most 0.025.
The reference program's roundings to bfloat16 on the way count: a program that leaves them out, or rounds other values in their place, can miss the bound.
Values may be sent and summed in bfloat16 or wider, within the bound.
A program may use at most 64 MiB of HBM per device.

```python
import jax
import jax.numpy as jnp
from jax import lax

D = 2048
HEADS = 32
NOPE = 128
ROPE = 64
DV = 128
QR = 512
KVR = 512
GRID_W = 64
CTX = 512
TOKENS = 6144


def draw_latent(key, part):
    noise = jax.random.normal(jax.random.fold_in(key, 11), (TOKENS, D), jnp.float32)
    rough = jax.random.uniform(jax.random.fold_in(key, 12), (1, D), jnp.float32, 0.7, 1.4)
    rising = 0.5 * jnp.exp(jnp.log(3.0) * jnp.arange(D, dtype=jnp.float32) / (D - 1))
    values = noise * rough * rising
    return jnp.clip(values, -12.0, 12.0).astype(jnp.bfloat16)


def draw_g_cq(key, part):
    return jax.random.uniform(jax.random.fold_in(key, 21), (QR,), jnp.float32, 0.5, 1.5)


def raised(drawn, stream_key, source, target, blocks, factor):
    def block_of(position):
        return (jnp.arange(drawn.shape[position]) // (drawn.shape[position] // blocks)).reshape((-1,) + (1,) * (drawn.ndim - 1 - position))

    near = jax.random.permutation(stream_key, blocks)[block_of(target)]
    far = (block_of(target) + blocks // 2) % blocks
    return jnp.where((block_of(source) == near) | (block_of(source) == far), factor * drawn, drawn)


def levels(rng, shape, split, least, largest):
    level = 1.0
    for position, blocks in split:
        draws = jax.random.uniform(jax.random.fold_in(jax.random.fold_in(rng, 6), position), (blocks,), jnp.float32, least / len(split), largest / len(split))
        level = level * jnp.repeat(jnp.exp(draws), shape[position] // blocks).reshape((-1,) + (1,) * (len(shape) - 1 - position))
    return level


def gaussian(rng, shape, scale, most, pieces=(), kind=jnp.bfloat16):
    result = jax.random.normal(rng, shape, jnp.float32) * scale
    if len(pieces) > 0:
        result = levels(rng, shape, pieces, -0.22, 0.18) * result
    return jnp.clip(result, min=-most, max=most).astype(kind)


def noise_with(stream_key, shape, width, most, shards, heavy, kind=jnp.bfloat16):
    drawn = width * jax.random.normal(stream_key, shape, jnp.float32)
    if shards:
        drawn = drawn * levels(stream_key, shape, shards, -0.22, 0.18)
    return jnp.clip(raised(drawn, jax.random.fold_in(stream_key, 3), *heavy), -most, most).astype(kind)


def setup_inputs(seed: int = 0) -> dict:
    arg_keys = jax.random.split(jax.random.key(seed), 16)
    latent = draw_latent(jax.random.fold_in(arg_keys[15], 71), 0)
    context = gaussian(arg_keys[1], (CTX, D), 1.0, 6.0, ((0, 16), (1, 32)))
    cond = gaussian(arg_keys[2], (D,), 1.0, 6.0, ((0, 16),))
    cond_ctx = gaussian(arg_keys[3], (D,), 1.0, 6.0, ((0, 16),))
    w_mod = gaussian(arg_keys[4], (D, 3, D), (D // 4) ** -0.5, 0.25, ((0, 16), (2, 32)))
    g_norm = jnp.clip(1.0 + 0.18 * jax.random.normal(arg_keys[5], (D,), jnp.float32), 0.1, 1.9)
    w_dq = gaussian(arg_keys[6], (D, QR), D ** -0.5, 0.125, ((0, 32),))
    w_dkv = gaussian(arg_keys[7], (D, KVR), D ** -0.5, 0.125, ((0, 32),))
    w_kr = gaussian(arg_keys[8], (D, ROPE), D ** -0.5, 0.125, ((0, 32),))
    g_cq = draw_g_cq(jax.random.fold_in(arg_keys[15], 71), 0)
    g_ckv = jnp.clip(1.0 + 0.18 * jax.random.normal(arg_keys[10], (KVR,), jnp.float32), 0.1, 1.9)
    w_uq = gaussian(arg_keys[11], (QR, HEADS, NOPE + ROPE), QR ** -0.5, 0.25, ((1, 32),))
    w_ukv = gaussian(arg_keys[12], (KVR, HEADS, NOPE + DV), KVR ** -0.5, 0.25, ((1, 32),))
    ctx_lift = jnp.clip(1.0 + 2.0 * jax.random.uniform(arg_keys[13], (HEADS,), jnp.float32) ** levels(arg_keys[13], (HEADS,), ((0, 32),), -0.2, 0.2), 1.0, 3.0)
    w_out = noise_with(arg_keys[14], (HEADS, DV, D), ((TOKENS + CTX) ** 0.5 * (2 * HEADS * DV) ** -0.5), 6.0, ((0, 32),), (0, 2, 32, 2.75))
    return {"latent": latent, "context": context, "cond": cond, "cond_ctx": cond_ctx, "w_mod": w_mod, "g_norm": g_norm, "w_dq": w_dq, "w_dkv": w_dkv, "w_kr": w_kr, "g_cq": g_cq, "g_ckv": g_ckv, "w_uq": w_uq, "w_ukv": w_ukv, "ctx_lift": ctx_lift, "w_out": w_out}


EPS = 1e-06
THETA = 10000.0

def tables(positions):
    row = (positions // GRID_W).astype(jnp.float32)
    col = (positions % GRID_W).astype(jnp.float32)
    half = ROPE // 2
    inverse = 1.0 / THETA ** (jnp.arange(0, half, 2, dtype=jnp.float32) / half)
    angle = jnp.concatenate([row[:, None] * inverse, col[:, None] * inverse], axis=-1)
    return (jnp.cos(angle), jnp.sin(angle))

def rotate(values, cosine, sine):
    shape = values.shape
    quarter = ROPE // 4
    parts = values.reshape(shape[:-1] + (2, 2, quarter))
    extra = (1,) * (len(shape) - 2)
    cosine = cosine.reshape((shape[0],) + extra + (2, quarter))
    sine = sine.reshape((shape[0],) + extra + (2, quarter))
    front_section = parts[..., 0, :]
    second = parts[..., 1, :]
    turned = jnp.stack([front_section * cosine - second * sine, front_section * sine + second * cosine], axis=-2)
    return turned.reshape(shape)

def modulated(values, gain, modulation):
    values = values.astype(jnp.float32)
    sumsq = lax.optimization_barrier(jnp.sum(values * values, axis=1))
    scaled = values * lax.rsqrt(sumsq / D + EPS)[:, None] * gain
    return (scaled * (1.0 + modulation[1]) + modulation[0]).astype(jnp.bfloat16)

def low_norm(values, gain):
    scale = lax.rsqrt(lax.optimization_barrier(jnp.mean(values * values, axis=-1, keepdims=True)) + EPS)
    return (values * scale * gain).astype(jnp.bfloat16)

def reference(latent, context, cond, cond_ctx, w_mod, g_norm, w_dq, w_dkv, w_kr, g_cq, g_ckv, w_uq, w_ukv, ctx_lift, w_out):
    signal = jnp.stack([jax.nn.silu(cond.astype(jnp.float32)), jax.nn.silu(cond_ctx.astype(jnp.float32))]).astype(jnp.bfloat16)
    modulation = jnp.dot(signal, w_mod.reshape(D, 3 * D), preferred_element_type=jnp.float32).reshape(2, 3, D)
    lat_h = modulated(latent, g_norm, modulation[0])
    ctx_h = modulated(context, g_norm, modulation[1])
    lat_q = jnp.dot(lat_h, w_dq, preferred_element_type=jnp.float32)
    lat_kv = jnp.dot(lat_h, w_dkv, preferred_element_type=jnp.float32)
    lat_rot = jnp.dot(lat_h, w_kr, preferred_element_type=jnp.float32)
    ctx_kv = jnp.dot(ctx_h, w_dkv, preferred_element_type=jnp.float32)
    ctx_rot = jnp.dot(ctx_h, w_kr, preferred_element_type=jnp.float32)
    positions = jnp.arange(TOKENS, dtype=jnp.int32)
    cosine, sine = tables(positions)
    cq_n = low_norm(lat_q, g_cq)
    ckv_n = low_norm(lat_kv, g_ckv)
    ctx_ckv_n = low_norm(ctx_kv, g_ckv)
    lat_kr = rotate(lat_rot, cosine, sine).astype(jnp.bfloat16)
    ctx_kr = ctx_rot.astype(jnp.bfloat16)
    query = jnp.dot(cq_n, w_uq.reshape(QR, HEADS * (NOPE + ROPE)), preferred_element_type=jnp.float32)
    query = query.reshape(TOKENS, HEADS, NOPE + ROPE)
    query = jnp.concatenate([query[..., :NOPE], rotate(query[..., NOPE:], cosine, sine)], axis=-1).astype(jnp.bfloat16)
    up_weight = w_ukv.reshape(KVR, HEADS * (NOPE + DV))
    lat_pairs = jnp.dot(ckv_n, up_weight, preferred_element_type=jnp.float32).astype(jnp.bfloat16)
    ctx_pairs = jnp.dot(ctx_ckv_n, up_weight, preferred_element_type=jnp.float32).astype(jnp.bfloat16)
    pairs = jnp.concatenate([ctx_pairs, lat_pairs], axis=0).reshape(CTX + TOKENS, HEADS, NOPE + DV)
    rope_keys = jnp.concatenate([ctx_kr, lat_kr], axis=0)
    key_index = jnp.arange(CTX + TOKENS, dtype=jnp.int32)
    scale = (NOPE + ROPE) ** (-0.5)

    def one_head(inputs):
        head_query, head_pairs, lift = inputs
        keys = jnp.concatenate([head_pairs[:, :NOPE], rope_keys], axis=1)
        raw_affinity_matrix = jnp.dot(head_query, keys.T, preferred_element_type=jnp.float32) * scale
        raw_affinity_matrix = raw_affinity_matrix + jnp.where(key_index < CTX, lift, 0.0 * lift)[None, :]
        peak = lax.optimization_barrier(jnp.max(raw_affinity_matrix, axis=1, keepdims=True))
        probs = jnp.exp(raw_affinity_matrix - peak)
        total = lax.optimization_barrier(jnp.sum(probs, axis=1))
        summed = jnp.dot(probs.astype(jnp.bfloat16), head_pairs[:, NOPE:], preferred_element_type=jnp.float32)
        return (summed / total[:, None]).astype(jnp.bfloat16)
    heads_out = lax.map(one_head, (jnp.transpose(query, (1, 0, 2)), jnp.transpose(pairs, (1, 0, 2)), ctx_lift))
    branch = jnp.einsum('hqd,hde->qe', heads_out.astype(jnp.float32), w_out.astype(jnp.float32))
    return (latent.astype(jnp.float32) + modulation[0, 2] * branch).astype(jnp.bfloat16)
```

```python
import functools

import jax
import jax.numpy as jnp
from jax import lax
from jax.experimental import pallas as pl
from jax.experimental.pallas import tpu as pltpu
from jax.sharding import Mesh
from jax.sharding import PartitionSpec as P

MESH = pl.DeviceIdType.MESH
D = 2048
NOPE = 128
ROPE = 64
DV = 128
GRID_W = 64
EPS = 1e-06
THETA = 10000.0
LOG2E = 1.4426950408889634
SCALE = (NOPE + ROPE) ** (-0.5)

BLOCK = 16
OWNERS = 13
SP = 16
CHUNKS = 4
REL = (0, 1, -1, 2, -2, 3, -3, 4, -4, 5, -5, 6, -6, 7, -7, 8)
FAR_FIRST = tuple(
    sorted(
        [(dy, dx) for dy in range(4) for dx in range(4) if dy or dx],
        key=lambda o: -(min(o[0], 4 - o[0]) + min(o[1], 4 - o[1])),
    )
)


def nn(lhs, rhs):
    return jnp.dot(lhs, rhs, preferred_element_type=jnp.float32)


def nt(lhs, rhs):
    return lax.dot_general(lhs, rhs, (((1,), (1,)), ((), ())), preferred_element_type=jnp.float32)


class Place:
    def __init__(self):
        self.z = lax.axis_index("sp")
        self.t = lax.axis_index("tp")
        self.p = lax.div(self.t, 2)
        self.c = lax.rem(self.t, 2)
        self.y = lax.div(self.p, 4)
        self.x = lax.rem(self.p, 4)
        self.a = self.x * (1 - self.c) + self.y * self.c
        self.b = self.y * (1 - self.c) + self.x * self.c

    def dev(self, a, b):
        p = (4 * b + a) * (1 - self.c) + (4 * a + b) * self.c
        return (self.z, 2 * p + self.c)

    def partner(self):
        return (self.z, 2 * self.p + 1 - self.c)


def around(i, by):
    return lax.rem(i + by + 4, 4)


def exists(a, b):
    return 4 * a + b < OWNERS


def send(src, dst, send_sem, recv_sem, device):
    copy = pltpu.make_async_remote_copy(
        src_ref=src,
        dst_ref=dst,
        send_sem=send_sem,
        recv_sem=recv_sem,
        device_id=device,
        device_id_type=MESH,
    )
    copy.start()


def arrived(ref, sem):
    pltpu.make_async_copy(ref, ref, sem).wait()


class PlaneGather:
    def __init__(self, at, buf, s1, r1, s2, r2, sd, rd):
        self.at = at
        self.buf = buf
        self.s1, self.r1, self.s2, self.r2, self.sd, self.rd = s1, r1, s2, r2, sd, rd
        self.offsets = (0, -1, 1, 2)

    def slot(self, k, a, b):
        return self.buf.at[k, self.at.c * 16 + 4 * a + b]

    def half(self, k, a, b, h):
        return self.buf.at[k, self.at.c * 16 + 4 * a + b, pl.ds(2 * h, 2)]

    def first_start(self, k):
        at = self.at

        @pl.when(exists(at.a, at.b))
        def _():
            own = self.slot(k, at.a, at.b)
            send(own, own, self.s1.at[k, 0], self.r1.at[k, 0], at.dev(around(at.a, 1), at.b))
            send(own, own, self.s1.at[k, 1], self.r1.at[k, 1], at.dev(around(at.a, -1), at.b))

    def first_forward(self, k):
        at = self.at
        for role, by in ((0, -1), (1, 1)):
            a = around(at.a, by)

            @pl.when(exists(a, at.b))
            def _():
                arrived(self.slot(k, a, at.b), self.r1.at[k, role])
                part = self.half(k, a, at.b, role)
                send(part, part, self.s1.at[k, 2 + role], self.r1.at[k, 2 + role], at.dev(around(at.a, -by), at.b))

    def first_end(self, k):
        at = self.at
        a = around(at.a, 2)

        @pl.when(exists(a, at.b))
        def _():
            for role in (0, 1):
                arrived(self.half(k, a, at.b, role), self.r1.at[k, 2 + role])

    def second_start(self, k, j):
        at = self.at
        a = around(at.a, self.offsets[j])

        @pl.when(exists(a, at.b))
        def _():
            own = self.slot(k, a, at.b)
            send(own, own, self.s2.at[k, j, 0], self.r2.at[k, j, 0], at.dev(at.a, around(at.b, 1)))
            send(own, own, self.s2.at[k, j, 1], self.r2.at[k, j, 1], at.dev(at.a, around(at.b, -1)))

    def second_forward(self, k, j):
        at = self.at
        a = around(at.a, self.offsets[j])
        for role, by in ((0, -1), (1, 1)):
            b = around(at.b, by)

            @pl.when(exists(a, b))
            def _():
                arrived(self.slot(k, a, b), self.r2.at[k, j, role])
                part = self.half(k, a, b, role)
                send(part, part, self.s2.at[k, j, 2 + role], self.r2.at[k, j, 2 + role], at.dev(at.a, around(at.b, -by)))

    def second_end(self, k, j):
        at = self.at
        a = around(at.a, self.offsets[j])
        b = around(at.b, 2)

        @pl.when(exists(a, b))
        def _():
            for role in (0, 1):
                arrived(self.half(k, a, b, role), self.r2.at[k, j, 2 + role])

        row = self.buf.at[k, pl.ds(at.c * 16 + 4 * a, 4)]
        send(row, row, self.sd.at[k, j], self.rd.at[k, j], at.partner())

    def other_core(self, k):
        at = self.at
        for j in range(4):
            a = around(at.b, self.offsets[j])
            arrived(self.buf.at[k, pl.ds((1 - at.c) * 16 + 4 * a, 4)], self.rd.at[k, j])

    def all_sent(self, k):
        at = self.at
        own = self.slot(k, 0, 0)
        part = self.half(k, 0, 0, 0)

        @pl.when(exists(at.a, at.b))
        def _():
            arrived(own, self.s1.at[k, 0])
            arrived(own, self.s1.at[k, 1])

        for role, by in ((0, -1), (1, 1)):

            @pl.when(exists(around(at.a, by), at.b))
            def _():
                arrived(part, self.s1.at[k, 2 + role])

        for j in range(4):
            a = around(at.a, self.offsets[j])

            @pl.when(exists(a, at.b))
            def _():
                arrived(own, self.s2.at[k, j, 0])
                arrived(own, self.s2.at[k, j, 1])

            for role, by in ((0, -1), (1, 1)):

                @pl.when(exists(a, around(at.b, by)))
                def _():
                    arrived(part, self.s2.at[k, j, 2 + role])

            arrived(self.buf.at[k, pl.ds(0, 4)], self.sd.at[k, j])


def main_kernel(
    q_ref,
    item_ref,
    lift_ref,
    latent_ref,
    gate_ref,
    w_uk_ref,
    w_uvt_ref,
    w_out_ref,
    out_ref,
    keys,
    peak,
    total,
    accum,
    w_both,
    heads,
    heads_in,
    pieces,
    pieces_in,
    sums,
    sums_in,
    zs,
    zr,
    s1,
    r1,
    s2,
    r2,
    sd,
    rd,
    ws,
    wr,
    hs,
    hr,
    ps,
    pr,
    xs,
    xr,
):
    at = Place()
    barrier = pltpu.get_barrier_semaphore()

    def greet_z(i, carry):
        pl.semaphore_signal(barrier, inc=1, device_id=(lax.rem(at.z + i, SP), at.t), device_id_type=MESH)
        return carry

    def greet_plane(i, carry):
        pl.semaphore_signal(barrier, inc=1, device_id=(at.z, lax.rem(at.t + i, 32)), device_id_type=MESH)
        return carry

    lax.fori_loop(1, SP, greet_z, 0)
    lax.fori_loop(1, 32, greet_plane, 0)
    pl.semaphore_wait(barrier, 46)

    send(w_out_ref, w_both, ws, wr, at.partner())

    own_slot = at.c * 16 + 4 * at.a + at.b

    @pl.when(exists(at.a, at.b))
    def _():
        keys[0, own_slot, 0] = item_ref[...]
        for n in range(1, SP):
            k, i = divmod(n, 4)
            send(
                item_ref,
                keys.at[k, own_slot, i],
                zs.at[k],
                zr.at[k],
                (lax.rem(at.z - REL[n] + SP, SP), at.t),
            )

    gather = PlaneGather(at, keys, s1, r1, s2, r2, sd, rd)

    def chunk_here(k):
        @pl.when(exists(at.a, at.b))
        def _():
            arrived(keys.at[k, own_slot], zr.at[k])

    peak[...] = jnp.full(peak.shape, -1e30, jnp.float32)
    total[...] = jnp.zeros(total.shape, jnp.float32)
    accum[...] = jnp.zeros(accum.shape, jnp.float32)
    query = q_ref[...]
    lift = lift_ref[0, 0] * LOG2E

    def attend(k, g):
        block = keys[k, pl.ds(g * 16, OWNERS)].reshape(OWNERS * 4 * BLOCK, 640)
        ckv = block[:, :512]
        key = jnp.concatenate([nn(ckv, w_uk_ref[...]).astype(jnp.bfloat16), block[:, 512:]], axis=1)
        value = nt(w_uvt_ref[...], ckv).astype(jnp.bfloat16)
        score = nt(key, query) * (SCALE * LOG2E)
        extra = jnp.where(g == 1, lift, 0.0)
        score = jnp.concatenate([score[: 11 * 4 * BLOCK], score[11 * 4 * BLOCK :] + extra], axis=0)
        fresh = jnp.maximum(peak[...], jnp.max(score, axis=0, keepdims=True))
        probs = jnp.exp2(score - fresh)
        fade = jnp.exp2(peak[...] - fresh)
        peak[...] = fresh
        total[...] = total[...] * fade + jnp.sum(probs, axis=0, keepdims=True)
        accum[...] = accum[...] * fade + nn(value, probs.astype(jnp.bfloat16))

    @pl.when(exists(at.a, at.b))
    def _():
        arrived(keys.at[0, own_slot, pl.ds(1, 3)], zr.at[0])

    gather.first_start(0)
    gather.second_start(0, 0)

    def step(k, carry):
        last = k == CHUNKS

        @pl.when(jnp.logical_not(last))
        def _():
            gather.first_forward(k)
            gather.second_start(k, 1)
            gather.second_start(k, 2)

        @pl.when(k > 0)
        def _():
            attend(k - 1, at.c)

        @pl.when(jnp.logical_not(last))
        def _():
            gather.first_end(k)
            gather.second_start(k, 3)
            gather.second_forward(k, 0)

        @pl.when(k < CHUNKS - 1)
        def _():
            chunk_here(k + 1)
            gather.first_start(k + 1)

        @pl.when(k > 0)
        def _():
            gather.other_core(k - 1)
            attend(k - 1, 1 - at.c)

        @pl.when(jnp.logical_not(last))
        def _():
            gather.second_forward(k, 1)
            gather.second_forward(k, 2)
            gather.second_end(k, 0)
            gather.second_forward(k, 3)

        @pl.when(k < CHUNKS - 1)
        def _():
            gather.second_start(k + 1, 0)

        @pl.when(jnp.logical_not(last))
        def _():
            gather.second_end(k, 1)
            gather.second_end(k, 2)
            gather.second_end(k, 3)

        return carry

    lax.fori_loop(0, CHUNKS + 1, step, 0)

    rows = heads_in.shape[0]
    heads[...] = jnp.transpose(accum[...] / total[...]).astype(jnp.bfloat16)
    theirs = heads.at[pl.ds((1 - at.c) * rows, rows)]
    send(theirs, heads_in, hs, hr, at.partner())
    arrived(w_both, wr)
    arrived(heads_in, hr)
    mine = heads[pl.ds(at.c * rows, rows), :]
    other = heads_in[...]

    def product(p):
        columns = pl.ds(pl.multiple_of(p * 128, 128), 128)
        return nn(mine, w_out_ref[:, columns]) + nn(other, w_both[:, columns])

    for n, (dy, dx) in enumerate(FAR_FIRST):
        p = 4 * around(at.y, dy) + around(at.x, dx)
        pieces[n] = product(p).astype(jnp.bfloat16)
        send(pieces.at[n], pieces_in.at[n], ps, pr, (at.z, 2 * p + at.c))
    here = product(at.p)
    arrived(pieces_in, pr)
    for n in range(15):
        here = here + pieces_in[n].astype(jnp.float32)
    sums[...] = here
    send(sums, sums_in, xs, xr, at.partner())
    gate = gate_ref[...]

    def finish(value, start):
        value = jnp.where(at.c == 0, value[:, :64], value[:, 64:])
        where = pl.ds(start, rows)
        out_ref[where, :] = (latent_ref[where, :].astype(jnp.float32) + gate * value).astype(jnp.bfloat16)

    finish(here, at.c * rows)
    arrived(sums_in, xr)
    finish(sums_in[...], (1 - at.c) * rows)

    arrived(w_both, ws)
    arrived(heads_in, hs)
    arrived(pieces_in, ps)
    arrived(sums_in, xs)

    @pl.when(exists(at.a, at.b))
    def _():
        arrived(keys.at[0, 0, pl.ds(1, 3)], zs.at[0])
        for k in range(1, CHUNKS):
            arrived(keys.at[k, 0], zs.at[k])

    def sent(k, carry):
        gather.all_sent(k)
        return carry

    lax.fori_loop(0, CHUNKS, sent, 0)


def main(q, item, lift, latent, gate, w_uk, w_uvt, w_out):
    rows = latent.shape[0]
    vmem = pl.BlockSpec(memory_space=pltpu.VMEM)
    smem = pl.BlockSpec(memory_space=pltpu.SMEM)
    dma = pltpu.SemaphoreType.DMA
    return pl.pallas_call(
        main_kernel,
        out_shape=jax.ShapeDtypeStruct((rows, 64), jnp.bfloat16),
        in_specs=[vmem, vmem, smem, vmem, vmem, vmem, vmem, vmem],
        out_specs=vmem,
        scratch_shapes=[
            pltpu.VMEM((CHUNKS, 32, 4, BLOCK, 640), jnp.bfloat16),
            pltpu.VMEM((1, rows), jnp.float32),
            pltpu.VMEM((1, rows), jnp.float32),
            pltpu.VMEM((DV, rows), jnp.float32),
            pltpu.VMEM((DV, D), jnp.bfloat16),
            pltpu.VMEM((rows, DV), jnp.bfloat16),
            pltpu.VMEM((rows // 2, DV), jnp.bfloat16),
            pltpu.VMEM((15, rows // 2, 128), jnp.bfloat16),
            pltpu.VMEM((15, rows // 2, 128), jnp.bfloat16),
            pltpu.VMEM((rows // 2, 128), jnp.float32),
            pltpu.VMEM((rows // 2, 128), jnp.float32),
            dma((CHUNKS,)),
            dma((CHUNKS,)),
            dma((CHUNKS, 4)),
            dma((CHUNKS, 4)),
            dma((CHUNKS, 4, 4)),
            dma((CHUNKS, 4, 4)),
            dma((CHUNKS, 4)),
            dma((CHUNKS, 4)),
            dma,
            dma,
            dma,
            dma,
            dma,
            dma,
            dma,
            dma,
        ],
        compiler_params=pltpu.CompilerParams(
            collective_id=0, has_side_effects=True, vmem_limit_bytes=56 * 1024 * 1024
        ),
        name="main",
    )(q, item, lift, latent, gate, w_uk, w_uvt, w_out)


def tables(positions):
    row = (positions // GRID_W).astype(jnp.float32)
    col = (positions % GRID_W).astype(jnp.float32)
    half = ROPE // 2
    inverse = 1.0 / THETA ** (jnp.arange(0, half, 2, dtype=jnp.float32) / half)
    angle = jnp.concatenate([row[:, None] * inverse, col[:, None] * inverse], axis=-1)
    return (jnp.cos(angle), jnp.sin(angle))


def rotate(values, cosine, sine):
    shape = values.shape
    quarter = ROPE // 4
    parts = values.reshape(shape[:-1] + (2, 2, quarter))
    cosine = cosine.reshape((shape[0], 2, quarter))
    sine = sine.reshape((shape[0], 2, quarter))
    front, second = parts[..., 0, :], parts[..., 1, :]
    turned = jnp.stack([front * cosine - second * sine, front * sine + second * cosine], axis=-2)
    return turned.reshape(shape)


def modulated(values, sumsq, gain, modulation):
    scaled = values * lax.rsqrt(sumsq / D + EPS)[:, None] * gain
    return (scaled * (1.0 + modulation[1]) + modulation[0]).astype(jnp.bfloat16)


def low_norm(values, gain):
    scale = lax.rsqrt(jnp.mean(values * values, axis=-1, keepdims=True) + EPS)
    return (values * scale * gain).astype(jnp.bfloat16)


def per_device(
    latent, context, cond, cond_ctx, w_mod, g_norm, w_dq, w_dkv, w_kr, g_cq, g_ckv, w_uq, w_ukv, ctx_lift, w_out
):
    rows = latent.shape[0]
    signal = jnp.stack(
        [jax.nn.silu(cond.astype(jnp.float32)), jax.nn.silu(cond_ctx.astype(jnp.float32))]
    ).astype(jnp.bfloat16)
    partial_mod = nn(signal, w_mod.reshape(w_mod.shape[0], -1))
    modulation = lax.psum(partial_mod.reshape(2, 3, -1), "sp")
    lat_f = latent.astype(jnp.float32)
    ctx_f = context.astype(jnp.float32)
    squares = lax.psum(jnp.concatenate([jnp.sum(lat_f * lat_f, axis=1), jnp.sum(ctx_f * ctx_f, axis=1)]), "tp")
    lat_h = modulated(lat_f, squares[:rows], g_norm, modulation[0])
    ctx_h = modulated(ctx_f, squares[rows:], g_norm, modulation[1])
    whole = nn(jnp.concatenate([lat_h, ctx_h], axis=0), jnp.concatenate([w_dq, w_dkv, w_kr], axis=1))
    whole = lax.psum(whole, "tp")
    positions = lax.axis_index("sp") * rows + jnp.arange(rows, dtype=jnp.int32)
    cosine, sine = tables(positions)
    cq_n = low_norm(whole[:rows, :512], g_cq)
    ckv_n = low_norm(whole[:, 512:1024], g_ckv)
    rot = whole[:, 1024:]
    rot = jnp.concatenate([rotate(rot[:rows], cosine, sine), rot[rows:]], axis=0).astype(jnp.bfloat16)
    kv = jnp.concatenate([ckv_n, rot, jnp.zeros_like(rot)], axis=1)
    query = nn(cq_n, w_uq[:, 0, :])
    query = jnp.concatenate(
        [query[:, :NOPE], rotate(query[:, NOPE:], cosine, sine), jnp.zeros((rows, 64), jnp.float32)], axis=1
    ).astype(jnp.bfloat16)
    at = Place()
    index = jnp.minimum(13 * at.c + 4 * at.a + at.b, 25)
    item = lax.dynamic_slice_in_dim(kv, index * BLOCK, BLOCK, axis=0)
    up = w_ukv[:, 0, :]
    return main(
        query,
        item,
        ctx_lift.reshape(1, 1),
        latent,
        modulation[0, 2][None, :],
        up[:, :NOPE],
        up[:, NOPE:].T,
        w_out[0],
    )


def solution(mesh):
    return jax.shard_map(
        per_device,
        mesh=mesh,
        in_specs=(
            P("sp", "tp"),
            P("sp", "tp"),
            P("sp"),
            P("sp"),
            P("sp", None, "tp"),
            P("tp"),
            P("tp", None),
            P("tp", None),
            P("tp", None),
            P(),
            P(),
            P(None, "tp", None),
            P(None, "tp", None),
            P("tp"),
            P("tp", None, None),
        ),
        out_specs=P("sp", "tp"),
        check_vma=False,
    )
```

```python
import numpy as np

import jax
import jax.numpy as jnp
from jax import lax
from jax.experimental import pallas as pl
from jax.experimental.pallas import tpu as pltpu

from jax.sharding import PartitionSpec as P

MESH = pl.DeviceIdType.MESH
D = 2048
NOPE = 128
ROPE = 64
DV = 128
GRID_W = 64
EPS = 1e-06
THETA = 10000.0
LOG2E = 1.4426950408889634
SCALE = (NOPE + ROPE) ** (-0.5)

BLOCK = 16
OWNERS = 13
SP = 16
CHUNKS = 4
REL = (0, 1, -1, 2, -2, 3, -3, 4, -4, 5, -5, 6, -6, 7, -7, 8)
FAR_FIRST = tuple(
    sorted(
        [(dy, dx) for dy in range(4) for dx in range(4) if dy or dx],
        key=lambda o: -(min(o[0], 4 - o[0]) + min(o[1], 4 - o[1])),
    )
)


def nn(lhs, rhs):
    return jnp.dot(lhs, rhs, preferred_element_type=jnp.float32)


def nt(lhs, rhs):
    return lax.dot_general(lhs, rhs, (((1,), (1,)), ((), ())), preferred_element_type=jnp.float32)


class Place:
    def __init__(self):
        self.z = lax.axis_index("sp")
        self.t = lax.axis_index("tp")
        self.p = lax.div(self.t, 2)
        self.c = lax.rem(self.t, 2)
        self.y = lax.div(self.p, 4)
        self.x = lax.rem(self.p, 4)
        self.a = self.x * (1 - self.c) + self.y * self.c
        self.b = self.y * (1 - self.c) + self.x * self.c

    def dev(self, a, b):
        p = (4 * b + a) * (1 - self.c) + (4 * a + b) * self.c
        return (self.z, 2 * p + self.c)

    def partner(self):
        return (self.z, 2 * self.p + 1 - self.c)


def around(i, by):
    return lax.rem(i + by + 4, 4)


def exists(a, b):
    return 4 * a + b < OWNERS


def send(src, dst, send_sem, recv_sem, device):
    copy = pltpu.make_async_remote_copy(
        src_ref=src,
        dst_ref=dst,
        send_sem=send_sem,
        recv_sem=recv_sem,
        device_id=device,
        device_id_type=MESH,
    )
    copy.start()


def arrived(ref, sem):
    pltpu.make_async_copy(ref, ref, sem).wait()


class PlaneGather:
    def __init__(self, at, buf, owners, part, sems):
        s1, r1, s2, r2, sd, rd = sems
        self.at = at
        self.buf = buf
        self.owners = owners
        self.part = part
        self.s1, self.r1, self.s2, self.r2, self.sd, self.rd = s1, r1, s2, r2, sd, rd
        self.offsets = (0, -1, 1, 2)

    def exists(self, a, b):
        return 4 * a + b < self.owners

    def slot(self, k, a, b):
        return self.buf.at[k, self.at.c * 16 + 4 * a + b]

    def half(self, k, a, b, h):
        return self.buf.at[k, self.at.c * 16 + 4 * a + b, pl.ds(self.part * h, self.part)]

    def first_start(self, k):
        at = self.at

        @pl.when(self.exists(at.a, at.b))
        def _():
            own = self.slot(k, at.a, at.b)
            send(own, own, self.s1.at[k, 0], self.r1.at[k, 0], at.dev(around(at.a, 1), at.b))
            send(own, own, self.s1.at[k, 1], self.r1.at[k, 1], at.dev(around(at.a, -1), at.b))

    def first_forward(self, k):
        at = self.at
        for role, by in ((0, -1), (1, 1)):
            a = around(at.a, by)

            @pl.when(self.exists(a, at.b))
            def _():
                arrived(self.slot(k, a, at.b), self.r1.at[k, role])
                part = self.half(k, a, at.b, role)
                send(part, part, self.s1.at[k, 2 + role], self.r1.at[k, 2 + role], at.dev(around(at.a, -by), at.b))

    def first_end(self, k):
        at = self.at
        a = around(at.a, 2)

        @pl.when(self.exists(a, at.b))
        def _():
            for role in (0, 1):
                arrived(self.half(k, a, at.b, role), self.r1.at[k, 2 + role])

    def second_start(self, k, j):
        at = self.at
        a = around(at.a, self.offsets[j])

        @pl.when(self.exists(a, at.b))
        def _():
            own = self.slot(k, a, at.b)
            send(own, own, self.s2.at[k, j, 0], self.r2.at[k, j, 0], at.dev(at.a, around(at.b, 1)))
            send(own, own, self.s2.at[k, j, 1], self.r2.at[k, j, 1], at.dev(at.a, around(at.b, -1)))

    def second_forward(self, k, j):
        at = self.at
        a = around(at.a, self.offsets[j])
        for role, by in ((0, -1), (1, 1)):
            b = around(at.b, by)

            @pl.when(self.exists(a, b))
            def _():
                arrived(self.slot(k, a, b), self.r2.at[k, j, role])
                part = self.half(k, a, b, role)
                send(part, part, self.s2.at[k, j, 2 + role], self.r2.at[k, j, 2 + role], at.dev(at.a, around(at.b, -by)))

    def second_end(self, k, j):
        at = self.at
        a = around(at.a, self.offsets[j])
        b = around(at.b, 2)

        @pl.when(self.exists(a, b))
        def _():
            for role in (0, 1):
                arrived(self.half(k, a, b, role), self.r2.at[k, j, 2 + role])

        row = self.buf.at[k, pl.ds(at.c * 16 + 4 * a, 4)]
        send(row, row, self.sd.at[k, j], self.rd.at[k, j], at.partner())

    def other_core(self, k):
        at = self.at
        for j in range(4):
            a = around(at.b, self.offsets[j])
            arrived(self.buf.at[k, pl.ds((1 - at.c) * 16 + 4 * a, 4)], self.rd.at[k, j])

    def all_sent(self, k):
        at = self.at
        own = self.slot(k, 0, 0)
        part = self.half(k, 0, 0, 0)

        @pl.when(self.exists(at.a, at.b))
        def _():
            arrived(own, self.s1.at[k, 0])
            arrived(own, self.s1.at[k, 1])

        for role, by in ((0, -1), (1, 1)):

            @pl.when(self.exists(around(at.a, by), at.b))
            def _():
                arrived(part, self.s1.at[k, 2 + role])

        for j in range(4):
            a = around(at.a, self.offsets[j])

            @pl.when(self.exists(a, at.b))
            def _():
                arrived(own, self.s2.at[k, j, 0])
                arrived(own, self.s2.at[k, j, 1])

            for role, by in ((0, -1), (1, 1)):

                @pl.when(self.exists(a, around(at.b, by)))
                def _():
                    arrived(part, self.s2.at[k, j, 2 + role])

            arrived(self.buf.at[k, pl.ds(0, 4)], self.sd.at[k, j])


def swapped(values):
    lane = lax.broadcasted_iota(jnp.int32, values.shape, 1)
    return jnp.where(lax.rem(lane, 32) < 16, pltpu.roll(values, 112, 1), pltpu.roll(values, 16, 1))


def low_norm(values, gain):
    scale = lax.rsqrt(jnp.mean(values * values, axis=-1, keepdims=True) + EPS)
    return (values * scale * gain).astype(jnp.bfloat16)


def main_kernel(
    latent_ref,
    context_ref,
    mod_ref,
    g_norm_ref,
    w_dq_ref,
    w_dkv_ref,
    w_kr_ref,
    g_cq_ref,
    g_ckv_ref,
    lift_ref,
    row_cos_ref,
    row_sin_ref,
    col_cos_ref,
    col_sin_ref,
    w_uq_hbm,
    w_ukv_hbm,
    w_out_hbm,
    out_ref,
    mod_in,
    mod_mine,
    mod_all,
    x_all,
    h_all,
    w_down,
    compressed,
    item,
    w_uq,
    w_up,
    w_uvt,
    w_out,
    query,
    keys,
    peak,
    total,
    accum,
    w_other,
    heads,
    heads_in,
    pieces,
    pieces_in,
    sums,
    sums_in,
    ms,
    mr,
    as_,
    ar,
    vs,
    vr,
    zs,
    zr,
    *rest,
):
    down_sems, cq_sems, key_sems = rest[0:6], rest[6:12], rest[12:18]
    ws, wr, hs, hr, ps, pr, xs, xr, l1, l2, l3 = rest[18:]
    at = Place()
    owner = exists(at.a, at.b)
    own_slot = at.c * 16 + 4 * at.a + at.b
    own_item = jnp.minimum(at.c * OWNERS + 4 * at.a + at.b, 25)
    in_context = own_item >= 24

    barrier = pltpu.get_barrier_semaphore()

    def greet_z(i, carry):
        pl.semaphore_signal(barrier, inc=1, device_id=(lax.rem(at.z + i, SP), at.t), device_id_type=MESH)
        return carry

    def greet_plane(i, carry):
        pl.semaphore_signal(barrier, inc=1, device_id=(at.z, lax.rem(at.t + i, 32)), device_id_type=MESH)
        return carry

    lax.fori_loop(1, SP, greet_z, 0)
    lax.fori_loop(1, 32, greet_plane, 0)

    loads = [
        pltpu.make_async_copy(w_uq_hbm, w_uq, l1),
        pltpu.make_async_copy(w_ukv_hbm, w_up, l2),
        pltpu.make_async_copy(w_out_hbm, w_out, l3),
    ]
    for load in loads:
        load.start()

    half_rows = w_dq_ref.shape[0] // 2
    for h in range(2):
        rows = pl.ds(h * half_rows, half_rows)
        w_down[0, own_slot, h, :, 0:512] = w_dq_ref[rows, :]
        w_down[0, own_slot, h, :, 512:1024] = w_dkv_ref[rows, :]
        w_down[0, own_slot, h, :, 1024:1152] = jnp.concatenate(
            [w_kr_ref[rows, :], jnp.zeros((half_rows, 64), jnp.bfloat16)], axis=1
        )
    mod_mine[...] = jnp.zeros(mod_mine.shape, jnp.float32)
    peak[...] = jnp.full(peak.shape, -1e30, jnp.float32)
    total[...] = jnp.zeros(total.shape, jnp.float32)
    accum[...] = jnp.zeros(accum.shape, jnp.float32)

    pl.semaphore_wait(barrier, 46)

    for n in range(1, SP):
        send(mod_ref, mod_in.at[n - 1], ms, mr, (lax.rem(at.z - REL[n] + SP, SP), at.t))

    down = PlaneGather(at, w_down, 16, 1, down_sems)
    down.first_start(0)
    down.second_start(0, 0)

    def give(i, source):
        c = lax.div(i, OWNERS)
        l = i - c * OWNERS
        a, b = lax.div(l, 4), lax.rem(l, 4)
        t = 2 * ((4 * b + a) * (1 - c) + (4 * a + b) * c) + c

        @pl.when(t != at.t)
        def _():
            send(source, x_all.at[own_slot], as_, ar, (at.z, t))

        @pl.when(t == at.t)
        def _():
            x_all[own_slot] = source[...]

    def give_latent(i, carry):
        give(i, latent_ref.at[pl.ds(pl.multiple_of(i * BLOCK, BLOCK), BLOCK)])
        return carry

    lax.fori_loop(0, 24, give_latent, 0)
    for i in (24, 25):
        give(jnp.int32(i), context_ref.at[pl.ds((i - 24) * BLOCK, BLOCK)])

    down.first_forward(0)
    down.second_start(0, 1)
    down.second_start(0, 2)
    loads[2].wait()
    send(w_out, w_other, ws, wr, at.partner())
    loads[1].wait()
    w_uvt[...] = jnp.transpose(w_up[:, NOPE:].astype(jnp.float32)).astype(jnp.bfloat16)
    down.first_end(0)
    down.second_start(0, 3)
    down.second_forward(0, 0)

    arrived(mod_in, mr)
    mod = mod_ref[...]
    for n in range(SP - 1):
        mod = mod + mod_in[n]
    mod_mine[:, 0:384] = mod
    mod_mine[:, 384:448] = g_norm_ref[...]
    mod_all[own_slot] = mod_mine[...]

    def tell(i, carry):
        send(mod_mine, mod_all.at[own_slot], vs, vr, (at.z, lax.rem(at.t + i, 32)))
        return carry

    lax.fori_loop(1, 32, tell, 0)

    for j in (1, 2, 3):
        down.second_forward(0, j)
    loads[0].wait()
    for j in range(4):
        down.second_end(0, j)

    @pl.when(owner)
    def _():
        arrived(x_all.at[pl.ds(0, 31)], ar)

    x = x_all[...].astype(jnp.float32)
    squares = jnp.sum(jnp.sum(x * x, axis=0), axis=1, keepdims=True)
    norm = lax.rsqrt(squares / D + EPS)
    arrived(mod_all.at[pl.ds(0, 31)], vr)
    for s in range(0, 32, 2):
        pair = []
        for slot in (s, s + 1):
            m = mod_all[slot]
            shift = jnp.where(in_context, m[:, 192:256], m[:, 0:64])
            scale = jnp.where(in_context, m[:, 256:320], m[:, 64:128])
            pair.append((x[slot] * norm * m[:, 384:448] * (1.0 + scale) + shift).astype(jnp.bfloat16))
        h_all[:, s * 64 : s * 64 + 128] = jnp.concatenate(pair, axis=1)
    down.other_core(0)
    low = nn(h_all[...], w_down[0].reshape(D, 1152))

    first_row = at.z * 6
    item_row = first_row + lax.div(jnp.minimum(own_item, 23), 4)
    item_col = pl.ds(pl.multiple_of(lax.rem(own_item, 4) * BLOCK, BLOCK), BLOCK)
    item_cos = jnp.where(in_context, 1.0, row_cos_ref[pl.ds(item_row, 1), :] + col_cos_ref[item_col, :])
    item_sin = jnp.where(in_context, 0.0, row_sin_ref[pl.ds(item_row, 1), :] + col_sin_ref[item_col, :])
    rotary = low[:, 1024:1152]
    rotary = rotary * item_cos + swapped(rotary) * item_sin
    item[:, 0:512] = low_norm(low[:, 512:1024], g_ckv_ref[...])
    item[:, 512:640] = rotary.astype(jnp.bfloat16)
    cq = low_norm(low[:, 0:512], g_cq_ref[...])
    compressed[0, own_slot, 0] = cq[:, 0:256]
    compressed[0, own_slot, 1] = cq[:, 256:512]

    @pl.when(owner)
    def _():
        keys[0, own_slot, 0] = item[...]
        for n in range(1, SP):
            k, i = divmod(n, 4)
            send(
                item,
                keys.at[k, own_slot, i],
                zs.at[k],
                zr.at[k],
                (lax.rem(at.z - REL[n] + SP, SP), at.t),
            )

    ask = PlaneGather(at, compressed, OWNERS, 1, cq_sems)
    gather = PlaneGather(at, keys, OWNERS, 2, key_sems)
    ask.first_start(0)
    ask.second_start(0, 0)
    ask.first_forward(0)
    ask.second_start(0, 1)
    ask.second_start(0, 2)

    def chunk_here(k):
        @pl.when(owner)
        def _():
            arrived(keys.at[k, own_slot], zr.at[k])

    lift = lift_ref[0, 0] * LOG2E

    def attend(k, g):
        block = keys[k, pl.ds(g * 16, OWNERS)].reshape(OWNERS * 4 * BLOCK, 640)
        ckv = block[:, :512]
        key = jnp.concatenate([nn(ckv, w_up[:, :NOPE]).astype(jnp.bfloat16), block[:, 512:]], axis=1)
        value = nt(w_uvt[...], ckv).astype(jnp.bfloat16)
        score = nt(key, query[...]) * (SCALE * LOG2E)
        extra = jnp.where(g == 1, lift, 0.0)
        score = jnp.concatenate([score[: 11 * 4 * BLOCK], score[11 * 4 * BLOCK :] + extra], axis=0)
        fresh = jnp.maximum(peak[...], jnp.max(score, axis=0, keepdims=True))
        probs = jnp.exp2(score - fresh)
        fade = jnp.exp2(peak[...] - fresh)
        peak[...] = fresh
        total[...] = total[...] * fade + jnp.sum(probs, axis=0, keepdims=True)
        accum[...] = accum[...] * fade + nn(value, probs.astype(jnp.bfloat16))

    @pl.when(owner)
    def _():
        arrived(keys.at[0, own_slot, pl.ds(1, 3)], zr.at[0])

    gather.first_start(0)
    ask.first_end(0)
    ask.second_start(0, 3)
    for j in range(4):
        ask.second_forward(0, j)
    gather.second_start(0, 0)
    for j in range(4):
        ask.second_end(0, j)

    def make_query():
        ask.other_core(0)
        pieces = [compressed[0, pl.ds(16 * c, 13 - 2 * c), h] for c in range(2) for h in range(2)]
        pieces = [piece.reshape(-1, 256) for piece in pieces]
        cq = jnp.concatenate(
            [jnp.concatenate(pieces[0:2], axis=1), jnp.concatenate(pieces[2:4], axis=1)], axis=0
        )
        query[:, 0:NOPE] = nn(cq, w_uq[:, 0:NOPE]).astype(jnp.bfloat16)
        turn = nn(cq, w_uq[:, NOPE:])
        turn = jnp.concatenate([turn, jnp.zeros_like(turn)], axis=1)
        for r in range(6):
            values = turn[64 * r : 64 * r + 64]
            cosine = row_cos_ref[pl.ds(first_row + r, 1), :] + col_cos_ref[...]
            sine = row_sin_ref[pl.ds(first_row + r, 1), :] + col_sin_ref[...]
            query[64 * r : 64 * r + 64, NOPE:] = (values * cosine + swapped(values) * sine).astype(jnp.bfloat16)

    def step(k, carry):
        last = k == CHUNKS

        @pl.when(jnp.logical_not(last))
        def _():
            gather.first_forward(k)
            gather.second_start(k, 1)
            gather.second_start(k, 2)

        @pl.when(k == 0)
        def _():
            make_query()

        @pl.when(k > 0)
        def _():
            attend(k - 1, at.c)

        @pl.when(jnp.logical_not(last))
        def _():
            gather.first_end(k)
            gather.second_start(k, 3)
            gather.second_forward(k, 0)

        @pl.when(k < CHUNKS - 1)
        def _():
            chunk_here(k + 1)
            gather.first_start(k + 1)

        @pl.when(k > 0)
        def _():
            gather.other_core(k - 1)
            attend(k - 1, 1 - at.c)

        @pl.when(jnp.logical_not(last))
        def _():
            gather.second_forward(k, 1)
            gather.second_forward(k, 2)
            gather.second_end(k, 0)
            gather.second_forward(k, 3)

        @pl.when(k < CHUNKS - 1)
        def _():
            gather.second_start(k + 1, 0)

        @pl.when(jnp.logical_not(last))
        def _():
            gather.second_end(k, 1)
            gather.second_end(k, 2)
            gather.second_end(k, 3)

        return carry

    lax.fori_loop(0, CHUNKS + 1, step, 0)

    rows = heads_in.shape[0]
    heads[...] = jnp.transpose(accum[...] / total[...]).astype(jnp.bfloat16)
    theirs = heads.at[pl.ds((1 - at.c) * rows, rows)]
    send(theirs, heads_in, hs, hr, at.partner())
    arrived(w_other, wr)
    arrived(heads_in, hr)
    mine = heads[pl.ds(at.c * rows, rows), :]
    other = heads_in[...]

    def product(p):
        columns = pl.ds(pl.multiple_of(p * 128, 128), 128)
        return nn(mine, w_out[:, columns]) + nn(other, w_other[:, columns])

    for n, (dy, dx) in enumerate(FAR_FIRST):
        p = 4 * around(at.y, dy) + around(at.x, dx)
        pieces[n] = product(p).astype(jnp.bfloat16)
        send(pieces.at[n], pieces_in.at[n], ps, pr, (at.z, 2 * p + at.c))
    here = product(at.p)
    arrived(pieces_in, pr)
    for n in range(15):
        here = here + pieces_in[n].astype(jnp.float32)
    sums[...] = here
    send(sums, sums_in, xs, xr, at.partner())
    gate = mod_mine[:, 128:192]

    def finish(value, start):
        value = jnp.where(at.c == 0, value[:, :64], value[:, 64:])
        where = pl.ds(start, rows)
        out_ref[where, :] = (latent_ref[where, :].astype(jnp.float32) + gate * value).astype(jnp.bfloat16)

    finish(here, at.c * rows)
    arrived(sums_in, xr)
    finish(sums_in[...], (1 - at.c) * rows)

    arrived(mod_in, ms)
    arrived(mod_all.at[pl.ds(0, 31)], vs)
    arrived(w_other, ws)
    arrived(heads_in, hs)
    arrived(pieces_in, ps)
    arrived(sums_in, xs)

    @pl.when(owner)
    def _():
        arrived(x_all.at[pl.ds(0, 25)], as_)
        arrived(keys.at[0, 0, pl.ds(1, 3)], zs.at[0])
        for k in range(1, CHUNKS):
            arrived(keys.at[k, 0], zs.at[k])

    @pl.when(jnp.logical_not(owner))
    def _():
        arrived(x_all.at[pl.ds(0, 26)], as_)

    down.all_sent(0)
    ask.all_sent(0)

    def sent(k, carry):
        gather.all_sent(k)
        return carry

    lax.fori_loop(0, CHUNKS, sent, 0)


def gather_sems(chunks):
    dma = pltpu.SemaphoreType.DMA
    return [
        dma((chunks, 4)),
        dma((chunks, 4)),
        dma((chunks, 4, 4)),
        dma((chunks, 4, 4)),
        dma((chunks, 4)),
        dma((chunks, 4)),
    ]


def turn_tables():
    half = ROPE // 2
    inverse = (np.float32(1.0) / np.float32(THETA) ** (np.arange(0, half, 2, dtype=np.float32) / np.float32(half))).astype(
        np.float32
    )

    def table(count, start):
        angle = (np.arange(count, dtype=np.float32)[:, None] * inverse).astype(np.float32)
        cosine, sine = np.cos(angle), np.sin(angle)
        whole_cos = np.zeros((count, 128), np.float32)
        whole_sin = np.zeros((count, 128), np.float32)
        whole_cos[:, start : start + 32] = np.concatenate([cosine, cosine], axis=1)
        whole_sin[:, start : start + 32] = np.concatenate([-sine, sine], axis=1)
        return whole_cos, whole_sin

    return table(6144 // GRID_W, 0) + table(GRID_W, 32)


def per_device(
    latent, context, cond, cond_ctx, w_mod, g_norm, w_dq, w_dkv, w_kr, g_cq, g_ckv, w_uq, w_ukv, ctx_lift, w_out
):
    rows = latent.shape[0]
    signal = jnp.stack(
        [jax.nn.silu(cond.astype(jnp.float32)), jax.nn.silu(cond_ctx.astype(jnp.float32))]
    ).astype(jnp.bfloat16)
    partial_mod = nn(signal, w_mod.reshape(w_mod.shape[0], -1)).reshape(1, 384)
    vmem = pl.BlockSpec(memory_space=pltpu.VMEM)
    smem = pl.BlockSpec(memory_space=pltpu.SMEM)
    hbm = pl.BlockSpec(memory_space=pltpu.HBM)
    dma = pltpu.SemaphoreType.DMA
    bf16, f32 = jnp.bfloat16, jnp.float32
    return pl.pallas_call(
        main_kernel,
        out_shape=jax.ShapeDtypeStruct((rows, 64), bf16),
        in_specs=[vmem] * 9 + [smem] + [vmem] * 4 + [hbm] * 3,
        out_specs=vmem,
        scratch_shapes=[
            pltpu.VMEM((SP - 1, 1, 384), f32),
            pltpu.VMEM((1, 512), f32),
            pltpu.VMEM((32, 1, 512), f32),
            pltpu.VMEM((32, BLOCK, 64), bf16),
            pltpu.VMEM((BLOCK, D), bf16),
            pltpu.VMEM((1, 32, 2, 32, 1152), bf16),
            pltpu.VMEM((1, 32, 2, BLOCK, 256), bf16),
            pltpu.VMEM((BLOCK, 640), bf16),
            pltpu.VMEM((512, NOPE + ROPE), bf16),
            pltpu.VMEM((512, NOPE + DV), bf16),
            pltpu.VMEM((DV, 512), bf16),
            pltpu.VMEM((DV, D), bf16),
            pltpu.VMEM((rows, 256), bf16),
            pltpu.VMEM((CHUNKS, 32, 4, BLOCK, 640), bf16),
            pltpu.VMEM((1, rows), f32),
            pltpu.VMEM((1, rows), f32),
            pltpu.VMEM((DV, rows), f32),
            pltpu.VMEM((DV, D), bf16),
            pltpu.VMEM((rows, DV), bf16),
            pltpu.VMEM((rows // 2, DV), bf16),
            pltpu.VMEM((15, rows // 2, 128), bf16),
            pltpu.VMEM((15, rows // 2, 128), bf16),
            pltpu.VMEM((rows // 2, 128), f32),
            pltpu.VMEM((rows // 2, 128), f32),
            dma,
            dma,
            dma,
            dma,
            dma,
            dma,
            dma((CHUNKS,)),
            dma((CHUNKS,)),
            *gather_sems(1),
            *gather_sems(1),
            *gather_sems(CHUNKS),
            *[dma] * 11,
        ],
        compiler_params=pltpu.CompilerParams(
            collective_id=0, has_side_effects=True, vmem_limit_bytes=56 * 1024 * 1024
        ),
        name="main",
    )(
        latent,
        context,
        partial_mod,
        g_norm[None, :],
        w_dq,
        w_dkv,
        w_kr,
        g_cq[None, :],
        g_ckv[None, :],
        ctx_lift.reshape(1, 1),
        *turn_tables(),
        w_uq[:, 0, :],
        w_ukv[:, 0, :],
        w_out[0],
    )


def solution(mesh):
    return jax.shard_map(
        per_device,
        mesh=mesh,
        in_specs=(
            P("sp", "tp"),
            P("sp", "tp"),
            P("sp"),
            P("sp"),
            P("sp", None, "tp"),
            P("tp"),
            P("tp", None),
            P("tp", None),
            P("tp", None),
            P(),
            P(),
            P(None, "tp", None),
            P(None, "tp", None),
            P("tp"),
            P("tp", None, None),
        ),
        out_specs=P("sp", "tp"),
        check_vma=False,
    )
```

```python
import numpy as np

import jax
import jax.numpy as jnp
from jax import lax
from jax.experimental import pallas as pl
from jax.experimental.pallas import tpu as pltpu

from jax.sharding import PartitionSpec as P

MESH = pl.DeviceIdType.MESH
D = 2048
NOPE = 128
ROPE = 64
DV = 128
GRID_W = 64
EPS = 1e-06
THETA = 10000.0
LOG2E = 1.4426950408889634
SCALE = (NOPE + ROPE) ** (-0.5)

BLOCK = 16
OWNERS = 13
SP = 16
CHUNKS = 4
REL = (0, 1, -1, 2, -2, 3, -3, 4, -4, 5, -5, 6, -6, 7, -7, 8)
FAR_FIRST = tuple(
    sorted(
        [(dy, dx) for dy in range(4) for dx in range(4) if dy or dx],
        key=lambda o: -(min(o[0], 4 - o[0]) + min(o[1], 4 - o[1])),
    )
)


def nn(lhs, rhs):
    return jnp.dot(lhs, rhs, preferred_element_type=jnp.float32)


def nt(lhs, rhs):
    return lax.dot_general(lhs, rhs, (((1,), (1,)), ((), ())), preferred_element_type=jnp.float32)


class Place:
    def __init__(self):
        self.z = lax.axis_index("sp")
        self.t = lax.axis_index("tp")
        self.p = lax.div(self.t, 2)
        self.c = lax.rem(self.t, 2)
        self.y = lax.div(self.p, 4)
        self.x = lax.rem(self.p, 4)
        self.a = self.x * (1 - self.c) + self.y * self.c
        self.b = self.y * (1 - self.c) + self.x * self.c

    def dev(self, a, b):
        p = (4 * b + a) * (1 - self.c) + (4 * a + b) * self.c
        return (self.z, 2 * p + self.c)

    def partner(self):
        return (self.z, 2 * self.p + 1 - self.c)


def around(i, by):
    return lax.rem(i + by + 4, 4)


def exists(a, b):
    return 4 * a + b < OWNERS


def send(src, dst, send_sem, recv_sem, device):
    copy = pltpu.make_async_remote_copy(
        src_ref=src,
        dst_ref=dst,
        send_sem=send_sem,
        recv_sem=recv_sem,
        device_id=device,
        device_id_type=MESH,
    )
    copy.start()


def arrived(ref, sem):
    pltpu.make_async_copy(ref, ref, sem).wait()


class PlaneGather:
    def __init__(self, at, buf, owners, way, sems):
        self.at = at
        self.buf = buf
        self.owners = owners
        self.way = way
        self.s1, self.r1, self.s2, self.r2, self.sd, self.rd = sems
        self.offsets = (0, -1, 1, 2)
        self.a, self.b = (at.a, at.b) if way == 0 else (at.b, at.a)

    def natural(self, a, b):
        return (a, b) if self.way == 0 else (b, a)

    def dev(self, a, b):
        return self.at.dev(*self.natural(a, b))

    def exists(self, a, b):
        a, b = self.natural(a, b)
        return 4 * a + b < self.owners

    def block(self, k, a, b, core=None):
        a, b = self.natural(a, b)
        core = self.at.c if core is None else core
        return self.buf.at[k, core * 16 + 4 * a + b, pl.ds(2 * self.way, 2)]

    def half(self, k, a, b, h):
        a, b = self.natural(a, b)
        return self.buf.at[k, self.at.c * 16 + 4 * a + b, pl.ds(2 * self.way + h, 1)]

    def across(self, k, a, b, j, m):
        block = self.block(k, a, b)
        send(block, block, self.sd.at[k, self.way, j, m], self.rd.at[k, self.way, j, m], self.at.partner())

    def first_start(self, k):
        @pl.when(self.exists(self.a, self.b))
        def _():
            own = self.block(k, self.a, self.b)
            for role, by in ((0, 1), (1, -1)):
                send(own, own, self.s1.at[k, self.way, role], self.r1.at[k, self.way, role], self.dev(around(self.a, by), self.b))

    def first_forward(self, k):
        for role, by in ((0, -1), (1, 1)):
            a = around(self.a, by)

            @pl.when(self.exists(a, self.b))
            def _():
                arrived(self.block(k, a, self.b), self.r1.at[k, self.way, role])
                part = self.half(k, a, self.b, role)
                send(
                    part,
                    part,
                    self.s1.at[k, self.way, 2 + role],
                    self.r1.at[k, self.way, 2 + role],
                    self.dev(around(self.a, -by), self.b),
                )

    def first_end(self, k):
        a = around(self.a, 2)

        @pl.when(self.exists(a, self.b))
        def _():
            for role in (0, 1):
                arrived(self.half(k, a, self.b, role), self.r1.at[k, self.way, 2 + role])

    def second_start(self, k, j):
        a = around(self.a, self.offsets[j])

        @pl.when(self.exists(a, self.b))
        def _():
            own = self.block(k, a, self.b)
            for role, by in ((0, 1), (1, -1)):
                send(
                    own, own, self.s2.at[k, self.way, j, role], self.r2.at[k, self.way, j, role], self.dev(self.a, around(self.b, by))
                )
            self.across(k, a, self.b, j, 0)

    def second_forward(self, k, j):
        a = around(self.a, self.offsets[j])
        for role, by in ((0, -1), (1, 1)):
            b = around(self.b, by)

            @pl.when(self.exists(a, b))
            def _():
                arrived(self.block(k, a, b), self.r2.at[k, self.way, j, role])
                part = self.half(k, a, b, role)
                send(
                    part,
                    part,
                    self.s2.at[k, self.way, j, 2 + role],
                    self.r2.at[k, self.way, j, 2 + role],
                    self.dev(self.a, around(self.b, -by)),
                )
                self.across(k, a, b, j, 1 + role)

    def second_end(self, k, j):
        a = around(self.a, self.offsets[j])
        b = around(self.b, 2)

        @pl.when(self.exists(a, b))
        def _():
            for role in (0, 1):
                arrived(self.half(k, a, b, role), self.r2.at[k, self.way, j, 2 + role])
            self.across(k, a, b, j, 3)

    def other_core(self, k):
        for j in range(4):
            a = around(self.b, self.offsets[j])
            for m in range(4):
                b = around(self.a, self.offsets[m])

                @pl.when(self.exists(a, b))
                def _():
                    arrived(self.block(k, a, b, 1 - self.at.c), self.rd.at[k, self.way, j, m])

    def all_sent(self, k):
        own = self.block(k, 0, 0)
        part = self.half(k, 0, 0, 0)

        @pl.when(self.exists(self.a, self.b))
        def _():
            arrived(own, self.s1.at[k, self.way, 0])
            arrived(own, self.s1.at[k, self.way, 1])

        for role, by in ((0, -1), (1, 1)):

            @pl.when(self.exists(around(self.a, by), self.b))
            def _():
                arrived(part, self.s1.at[k, self.way, 2 + role])

        for j in range(4):
            a = around(self.a, self.offsets[j])

            @pl.when(self.exists(a, self.b))
            def _():
                arrived(own, self.s2.at[k, self.way, j, 0])
                arrived(own, self.s2.at[k, self.way, j, 1])
                arrived(own, self.sd.at[k, self.way, j, 0])

            for role, by in ((0, -1), (1, 1)):

                @pl.when(self.exists(a, around(self.b, by)))
                def _():
                    arrived(part, self.s2.at[k, self.way, j, 2 + role])
                    arrived(own, self.sd.at[k, self.way, j, 1 + role])

            @pl.when(self.exists(a, around(self.b, 2)))
            def _():
                arrived(own, self.sd.at[k, self.way, j, 3])


class BothWays:
    def __init__(self, at, buf, owners, sems):
        self.ways = [PlaneGather(at, buf, owners, way, sems) for way in range(2)]

    def __getattr__(self, name):
        def call(*args):
            for way in self.ways:
                getattr(way, name)(*args)

        return call


def swapped(values):
    lane = lax.broadcasted_iota(jnp.int32, values.shape, 1)
    return jnp.where(lax.rem(lane, 32) < 16, pltpu.roll(values, 112, 1), pltpu.roll(values, 16, 1))


def low_norm(values, gain):
    scale = lax.rsqrt(jnp.mean(values * values, axis=-1, keepdims=True) + EPS)
    return (values * scale * gain).astype(jnp.bfloat16)


def main_kernel(
    latent_ref,
    context_ref,
    cond_ref,
    cond_ctx_ref,
    w_mod_ref,
    g_norm_ref,
    w_dq_ref,
    w_dkv_ref,
    w_kr_ref,
    g_cq_ref,
    g_ckv_ref,
    lift_ref,
    row_cos_ref,
    row_sin_ref,
    col_cos_ref,
    col_sin_ref,
    w_uq_hbm,
    w_ukv_hbm,
    w_out_hbm,
    out_ref,
    latent,
    mod_part,
    mod_in,
    mod_mine,
    mod_all,
    x_all,
    h_all,
    w_down,
    compressed,
    item,
    w_uq,
    w_up,
    w_uvt,
    w_out,
    query,
    keys,
    peak,
    total,
    accum,
    w_other,
    heads,
    heads_in,
    pieces,
    pieces_in,
    sums,
    sums_in,
    ms,
    mr,
    as_,
    ar,
    vs,
    vr,
    zs,
    zr,
    *rest,
):
    down_sems, cq_sems, key_sems = rest[0:6], rest[6:12], rest[12:18]
    ws, wr, hs, hr, ps, pr, xs, xr, l1, l2, l3 = rest[18:]
    at = Place()
    owner = exists(at.a, at.b)
    own_slot = at.c * 16 + 4 * at.a + at.b
    own_item = jnp.minimum(at.c * OWNERS + 4 * at.a + at.b, 25)
    in_context = own_item >= 24

    barrier = pltpu.get_barrier_semaphore()

    def greet_z(i, carry):
        pl.semaphore_signal(barrier, inc=1, device_id=(lax.rem(at.z + i, SP), at.t), device_id_type=MESH)
        return carry

    def greet_plane(i, carry):
        pl.semaphore_signal(barrier, inc=1, device_id=(at.z, lax.rem(at.t + i, 32)), device_id_type=MESH)
        return carry

    lax.fori_loop(1, SP, greet_z, 0)
    lax.fori_loop(1, 32, greet_plane, 0)

    loads = [
        pltpu.make_async_copy(w_uq_hbm, w_uq, l1),
        pltpu.make_async_copy(w_ukv_hbm, w_up, l2),
        pltpu.make_async_copy(w_out_hbm, w_out, l3),
    ]
    for load in loads:
        load.start()

    for n in range(4):
        rows = pl.ds(n * 16, 16)
        w_down[0, own_slot, n, :, 0:512] = w_dq_ref[rows, :]
        w_down[0, own_slot, n, :, 512:1024] = w_dkv_ref[rows, :]
        w_down[0, own_slot, n, :, 1024:1152] = jnp.concatenate(
            [w_kr_ref[rows, :], jnp.zeros((16, 64), jnp.bfloat16)], axis=1
        )
    latent[...] = jnp.transpose(latent_ref[...].astype(jnp.float32)).astype(jnp.bfloat16)
    signal = jnp.concatenate([cond_ref[...], cond_ctx_ref[...], jnp.zeros((6, 128), jnp.bfloat16)], axis=0)
    signal = jax.nn.silu(signal.astype(jnp.float32)).astype(jnp.bfloat16)
    partial_mod = nt(signal, w_mod_ref[...])
    mod_part[:, 0:192] = partial_mod[0:1]
    mod_part[:, 192:384] = partial_mod[1:2]
    mod_mine[...] = jnp.zeros(mod_mine.shape, jnp.float32)
    peak[...] = jnp.full(peak.shape, -1e30, jnp.float32)
    total[...] = jnp.zeros(total.shape, jnp.float32)
    accum[...] = jnp.zeros(accum.shape, jnp.float32)

    pl.semaphore_wait(barrier, 46)

    for n in range(1, SP):
        send(mod_part, mod_in.at[n - 1], ms, mr, (lax.rem(at.z - REL[n] + SP, SP), at.t))

    down = BothWays(at, w_down, 16, down_sems)
    down.first_start(0)
    down.second_start(0, 0)

    def give(i, source):
        c = lax.div(i, OWNERS)
        l = i - c * OWNERS
        a, b = lax.div(l, 4), lax.rem(l, 4)
        t = 2 * ((4 * b + a) * (1 - c) + (4 * a + b) * c) + c

        @pl.when(t != at.t)
        def _():
            send(source, x_all.at[own_slot], as_, ar, (at.z, t))

        @pl.when(t == at.t)
        def _():
            x_all[own_slot] = source[...]

    def give_latent(i, carry):
        give(i, latent.at[pl.ds(pl.multiple_of(i * BLOCK, BLOCK), BLOCK)])
        return carry

    lax.fori_loop(0, 24, give_latent, 0)
    for i in (24, 25):
        give(jnp.int32(i), context_ref.at[pl.ds((i - 24) * BLOCK, BLOCK)])

    down.first_forward(0)
    down.second_start(0, 1)
    down.second_start(0, 2)
    loads[2].wait()
    send(w_out, w_other, ws, wr, at.partner())
    loads[1].wait()
    w_uvt[...] = jnp.transpose(w_up[:, NOPE:].astype(jnp.float32)).astype(jnp.bfloat16)
    down.first_end(0)
    down.second_start(0, 3)
    down.second_forward(0, 0)

    arrived(mod_in, mr)
    mod = mod_part[...]
    for n in range(SP - 1):
        mod = mod + mod_in[n]
    mod_mine[:, 0:384] = mod
    mod_mine[:, 384:448] = g_norm_ref[...]
    mod_all[own_slot] = mod_mine[...]

    def tell(i, carry):
        send(mod_mine, mod_all.at[own_slot], vs, vr, (at.z, lax.rem(at.t + i, 32)))
        return carry

    lax.fori_loop(1, 32, tell, 0)

    for j in (1, 2, 3):
        down.second_forward(0, j)
    loads[0].wait()
    for j in range(4):
        down.second_end(0, j)

    @pl.when(owner)
    def _():
        arrived(x_all.at[pl.ds(0, 31)], ar)

    x = x_all[...].astype(jnp.float32)
    squares = jnp.sum(jnp.sum(x * x, axis=0), axis=1, keepdims=True)
    norm = lax.rsqrt(squares / D + EPS)
    arrived(mod_all.at[pl.ds(0, 31)], vr)
    for s in range(0, 32, 2):
        pair = []
        for slot in (s, s + 1):
            m = mod_all[slot]
            shift = jnp.where(in_context, m[:, 192:256], m[:, 0:64])
            scale = jnp.where(in_context, m[:, 256:320], m[:, 64:128])
            pair.append((x[slot] * norm * m[:, 384:448] * (1.0 + scale) + shift).astype(jnp.bfloat16))
        h_all[:, s * 64 : s * 64 + 128] = jnp.concatenate(pair, axis=1)
    down.other_core(0)
    low = nn(h_all[...], w_down[0].reshape(D, 1152))

    first_row = at.z * 6
    item_row = first_row + lax.div(jnp.minimum(own_item, 23), 4)
    item_col = pl.ds(pl.multiple_of(lax.rem(own_item, 4) * BLOCK, BLOCK), BLOCK)
    item_cos = jnp.where(in_context, 1.0, row_cos_ref[pl.ds(item_row, 1), :] + col_cos_ref[item_col, :])
    item_sin = jnp.where(in_context, 0.0, row_sin_ref[pl.ds(item_row, 1), :] + col_sin_ref[item_col, :])
    rotary = low[:, 1024:1152]
    rotary = rotary * item_cos + swapped(rotary) * item_sin
    item[:, 0:512] = low_norm(low[:, 512:1024], g_ckv_ref[...])
    item[:, 512:640] = rotary.astype(jnp.bfloat16)
    cq = low_norm(low[:, 0:512], g_cq_ref[...])
    for n in range(4):
        compressed[0, own_slot, n] = cq[:, 128 * n : 128 * n + 128]

    @pl.when(owner)
    def _():
        keys[0, own_slot, 0] = item[...]
        for n in range(1, SP):
            k, i = divmod(n, 4)
            send(
                item,
                keys.at[k, own_slot, i],
                zs.at[k],
                zr.at[k],
                (lax.rem(at.z - REL[n] + SP, SP), at.t),
            )

    ask = BothWays(at, compressed, OWNERS, cq_sems)
    gather = BothWays(at, keys, OWNERS, key_sems)
    ask.first_start(0)
    ask.second_start(0, 0)
    ask.first_forward(0)
    ask.second_start(0, 1)
    ask.second_start(0, 2)

    def chunk_here(k):
        @pl.when(owner)
        def _():
            arrived(keys.at[k, own_slot], zr.at[k])

    lift = lift_ref[0, 0] * LOG2E

    def attend(k, g):
        block = keys[k, pl.ds(g * 16, OWNERS)].reshape(OWNERS * 4 * BLOCK, 640)
        ckv = block[:, :512]
        key = jnp.concatenate([nn(ckv, w_up[:, :NOPE]).astype(jnp.bfloat16), block[:, 512:]], axis=1)
        value = nt(w_uvt[...], ckv).astype(jnp.bfloat16)
        score = nt(key, query[...]) * (SCALE * LOG2E)
        extra = jnp.where(g == 1, lift, 0.0)
        score = jnp.concatenate([score[: 11 * 4 * BLOCK], score[11 * 4 * BLOCK :] + extra], axis=0)
        fresh = jnp.maximum(peak[...], jnp.max(score, axis=0, keepdims=True))
        probs = jnp.exp2(score - fresh)
        fade = jnp.exp2(peak[...] - fresh)
        peak[...] = fresh
        total[...] = total[...] * fade + jnp.sum(probs, axis=0, keepdims=True)
        accum[...] = accum[...] * fade + nn(value, probs.astype(jnp.bfloat16))

    @pl.when(owner)
    def _():
        arrived(keys.at[0, own_slot, pl.ds(1, 3)], zr.at[0])

    gather.first_start(0)
    ask.first_end(0)
    ask.second_start(0, 3)
    for j in range(4):
        ask.second_forward(0, j)
    gather.second_start(0, 0)
    for j in range(4):
        ask.second_end(0, j)

    def make_query():
        ask.other_core(0)
        cq = jnp.concatenate(
            [
                jnp.concatenate([compressed[0, pl.ds(16 * c, 13 - 2 * c), n].reshape(-1, 128) for n in range(4)], axis=1)
                for c in range(2)
            ],
            axis=0,
        )
        query[:, 0:NOPE] = nt(cq, w_uq[0:NOPE, :]).astype(jnp.bfloat16)
        turn = nt(cq, w_uq[NOPE:, :])
        turn = jnp.concatenate([turn, jnp.zeros_like(turn)], axis=1)
        for r in range(6):
            values = turn[64 * r : 64 * r + 64]
            cosine = row_cos_ref[pl.ds(first_row + r, 1), :] + col_cos_ref[...]
            sine = row_sin_ref[pl.ds(first_row + r, 1), :] + col_sin_ref[...]
            query[64 * r : 64 * r + 64, NOPE:] = (values * cosine + swapped(values) * sine).astype(jnp.bfloat16)

    def step(k, carry):
        last = k == CHUNKS

        @pl.when(jnp.logical_not(last))
        def _():
            gather.first_forward(k)
            gather.second_start(k, 1)
            gather.second_start(k, 2)

        @pl.when(k == 0)
        def _():
            make_query()

        @pl.when(k > 0)
        def _():
            attend(k - 1, at.c)

        @pl.when(jnp.logical_not(last))
        def _():
            gather.first_end(k)
            gather.second_start(k, 3)
            gather.second_forward(k, 0)

        @pl.when(k < CHUNKS - 1)
        def _():
            chunk_here(k + 1)
            gather.first_start(k + 1)

        @pl.when(k > 0)
        def _():
            gather.other_core(k - 1)
            attend(k - 1, 1 - at.c)

        @pl.when(jnp.logical_not(last))
        def _():
            gather.second_forward(k, 1)
            gather.second_forward(k, 2)
            gather.second_end(k, 0)
            gather.second_forward(k, 3)

        @pl.when(k < CHUNKS - 1)
        def _():
            gather.second_start(k + 1, 0)

        @pl.when(jnp.logical_not(last))
        def _():
            gather.second_end(k, 1)
            gather.second_end(k, 2)
            gather.second_end(k, 3)

        return carry

    lax.fori_loop(0, CHUNKS + 1, step, 0)

    rows = heads_in.shape[0]
    heads[...] = jnp.transpose(accum[...] / total[...]).astype(jnp.bfloat16)
    theirs = heads.at[pl.ds((1 - at.c) * rows, rows)]
    send(theirs, heads_in, hs, hr, at.partner())
    arrived(w_other, wr)
    arrived(heads_in, hr)
    mine = heads[pl.ds(at.c * rows, rows), :]
    other = heads_in[...]

    def product(p):
        columns = pl.ds(pl.multiple_of(p * 128, 128), 128)
        return nn(mine, w_out[:, columns]) + nn(other, w_other[:, columns])

    for n, (dy, dx) in enumerate(FAR_FIRST):
        p = 4 * around(at.y, dy) + around(at.x, dx)
        pieces[n] = product(p).astype(jnp.bfloat16)
        send(pieces.at[n], pieces_in.at[n], ps, pr, (at.z, 2 * p + at.c))
    here = product(at.p)
    arrived(pieces_in, pr)
    for n in range(15):
        here = here + pieces_in[n].astype(jnp.float32)
    sums[...] = here
    send(sums, sums_in, xs, xr, at.partner())
    gate = mod_mine[:, 128:192]

    def columns_here(value):
        return gate * jnp.where(at.c == 0, value[:, :64], value[:, 64:])

    here = columns_here(here)
    arrived(sums_in, xr)
    there = columns_here(sums_in[...])
    branch = jnp.concatenate([jnp.where(at.c == 0, here, there), jnp.where(at.c == 0, there, here)], axis=0)
    out_ref[...] = (latent_ref[...].astype(jnp.float32) + jnp.transpose(branch)).astype(jnp.bfloat16)

    arrived(mod_in, ms)
    arrived(mod_all.at[pl.ds(0, 31)], vs)
    arrived(w_other, ws)
    arrived(heads_in, hs)
    arrived(pieces_in, ps)
    arrived(sums_in, xs)

    @pl.when(owner)
    def _():
        arrived(x_all.at[pl.ds(0, 25)], as_)
        arrived(keys.at[0, 0, pl.ds(1, 3)], zs.at[0])
        for k in range(1, CHUNKS):
            arrived(keys.at[k, 0], zs.at[k])

    @pl.when(jnp.logical_not(owner))
    def _():
        arrived(x_all.at[pl.ds(0, 26)], as_)

    down.all_sent(0)
    ask.all_sent(0)

    def sent(k, carry):
        gather.all_sent(k)
        return carry

    lax.fori_loop(0, CHUNKS, sent, 0)


def gather_sems(chunks):
    dma = pltpu.SemaphoreType.DMA
    few, many = dma((chunks, 2, 4)), dma((chunks, 2, 4, 4))
    return [few, few, many, many, many, many]


def turn_tables():
    half = ROPE // 2
    inverse = (np.float32(1.0) / np.float32(THETA) ** (np.arange(0, half, 2, dtype=np.float32) / np.float32(half))).astype(
        np.float32
    )

    def table(count, start):
        angle = (np.arange(count, dtype=np.float32)[:, None] * inverse).astype(np.float32)
        cosine, sine = np.cos(angle), np.sin(angle)
        whole_cos = np.zeros((count, 128), np.float32)
        whole_sin = np.zeros((count, 128), np.float32)
        whole_cos[:, start : start + 32] = np.concatenate([cosine, cosine], axis=1)
        whole_sin[:, start : start + 32] = np.concatenate([-sine, sine], axis=1)
        return whole_cos, whole_sin

    return table(6144 // GRID_W, 0) + table(GRID_W, 32)


def per_device(
    latent, context, cond, cond_ctx, w_mod, g_norm, w_dq, w_dkv, w_kr, g_cq, g_ckv, w_uq, w_ukv, ctx_lift, w_out
):
    rows = latent.shape[0]
    vmem = pl.BlockSpec(memory_space=pltpu.VMEM)
    smem = pl.BlockSpec(memory_space=pltpu.SMEM)
    hbm = pl.BlockSpec(memory_space=pltpu.HBM)
    dma = pltpu.SemaphoreType.DMA
    bf16, f32 = jnp.bfloat16, jnp.float32
    return pl.pallas_call(
        main_kernel,
        out_shape=jax.ShapeDtypeStruct((64, rows), bf16),
        in_specs=[vmem] * 11 + [smem] + [vmem] * 4 + [hbm] * 3,
        out_specs=vmem,
        scratch_shapes=[
            pltpu.VMEM((rows, 64), bf16),
            pltpu.VMEM((1, 384), f32),
            pltpu.VMEM((SP - 1, 1, 384), f32),
            pltpu.VMEM((1, 512), f32),
            pltpu.VMEM((32, 1, 512), f32),
            pltpu.VMEM((32, BLOCK, 64), bf16),
            pltpu.VMEM((BLOCK, D), bf16),
            pltpu.VMEM((1, 32, 4, 16, 1152), bf16),
            pltpu.VMEM((1, 32, 4, BLOCK, 128), bf16),
            pltpu.VMEM((BLOCK, 640), bf16),
            pltpu.VMEM((NOPE + ROPE, 512), bf16),
            pltpu.VMEM((512, NOPE + DV), bf16),
            pltpu.VMEM((DV, 512), bf16),
            pltpu.VMEM((DV, D), bf16),
            pltpu.VMEM((rows, 256), bf16),
            pltpu.VMEM((CHUNKS, 32, 4, BLOCK, 640), bf16),
            pltpu.VMEM((1, rows), f32),
            pltpu.VMEM((1, rows), f32),
            pltpu.VMEM((DV, rows), f32),
            pltpu.VMEM((DV, D), bf16),
            pltpu.VMEM((rows, DV), bf16),
            pltpu.VMEM((rows // 2, DV), bf16),
            pltpu.VMEM((15, rows // 2, 128), bf16),
            pltpu.VMEM((15, rows // 2, 128), bf16),
            pltpu.VMEM((rows // 2, 128), f32),
            pltpu.VMEM((rows // 2, 128), f32),
            dma,
            dma,
            dma,
            dma,
            dma,
            dma,
            dma((CHUNKS,)),
            dma((CHUNKS,)),
            *gather_sems(1),
            *gather_sems(1),
            *gather_sems(CHUNKS),
            *[dma] * 11,
        ],
        compiler_params=pltpu.CompilerParams(
            collective_id=0, has_side_effects=True, vmem_limit_bytes=56 * 1024 * 1024
        ),
        name="main",
    )(
        latent.T,
        context,
        cond[None, :],
        cond_ctx[None, :],
        jnp.transpose(w_mod, (1, 2, 0)).reshape(192, 128),
        g_norm[None, :],
        w_dq,
        w_dkv,
        w_kr,
        g_cq[None, :],
        g_ckv[None, :],
        ctx_lift.reshape(1, 1),
        *turn_tables(),
        w_uq[:, 0, :].T,
        w_ukv[:, 0, :],
        w_out[0],
    ).T


def solution(mesh):
    return jax.shard_map(
        per_device,
        mesh=mesh,
        in_specs=(
            P("sp", "tp"),
            P("sp", "tp"),
            P("sp"),
            P("sp"),
            P("sp", None, "tp"),
            P("tp"),
            P("tp", None),
            P("tp", None),
            P("tp", None),
            P(),
            P(),
            P(None, "tp", None),
            P(None, "tp", None),
            P("tp"),
            P("tp", None, None),
        ),
        out_specs=P("sp", "tp"),
        check_vma=False,
    )
```

```python
import numpy as np

import jax
import jax.numpy as jnp
from jax import lax
from jax.experimental import pallas as pl
from jax.experimental.pallas import tpu as pltpu

from jax.sharding import PartitionSpec as P

MESH = pl.DeviceIdType.MESH
D = 2048
NOPE = 128
ROPE = 64
DV = 128
GRID_W = 64
EPS = 1e-06
THETA = 10000.0
LOG2E = 1.4426950408889634
SCALE = (NOPE + ROPE) ** (-0.5)

BLOCK = 16
OWNERS = 13
SP = 16
CHUNKS = 4
REL = (0, 1, -1, 2, -2, 3, -3, 4, -4, 5, -5, 6, -6, 7, -7, 8)
FAR_FIRST = tuple(
    sorted(
        [(dy, dx) for dy in range(4) for dx in range(4) if dy or dx],
        key=lambda o: -(min(o[0], 4 - o[0]) + min(o[1], 4 - o[1])),
    )
)


def nn(lhs, rhs):
    return jnp.dot(lhs, rhs, preferred_element_type=jnp.float32)


def nt(lhs, rhs):
    return lax.dot_general(lhs, rhs, (((1,), (1,)), ((), ())), preferred_element_type=jnp.float32)


class Place:
    def __init__(self):
        self.z = lax.axis_index("sp")
        self.t = lax.axis_index("tp")
        self.p = lax.div(self.t, 2)
        self.c = lax.rem(self.t, 2)
        self.y = lax.div(self.p, 4)
        self.x = lax.rem(self.p, 4)
        self.a = self.x * (1 - self.c) + self.y * self.c
        self.b = self.y * (1 - self.c) + self.x * self.c

    def dev(self, a, b):
        p = (4 * b + a) * (1 - self.c) + (4 * a + b) * self.c
        return (self.z, 2 * p + self.c)

    def partner(self):
        return (self.z, 2 * self.p + 1 - self.c)


def around(i, by):
    return lax.rem(i + by + 4, 4)


def exists(a, b):
    return 4 * a + b < OWNERS


def send(src, dst, send_sem, recv_sem, device):
    copy = pltpu.make_async_remote_copy(
        src_ref=src,
        dst_ref=dst,
        send_sem=send_sem,
        recv_sem=recv_sem,
        device_id=device,
        device_id_type=MESH,
    )
    copy.start()


def arrived(ref, sem):
    pltpu.make_async_copy(ref, ref, sem).wait()


class PlaneGather:
    def __init__(self, at, buf, owners, way, sems):
        self.at = at
        self.buf = buf
        self.owners = owners
        self.way = way
        self.s1, self.r1, self.s2, self.r2, self.sd, self.rd = sems
        self.offsets = (0, -1, 1, 2)
        self.a, self.b = (at.a, at.b) if way == 0 else (at.b, at.a)

    def natural(self, a, b):
        return (a, b) if self.way == 0 else (b, a)

    def dev(self, a, b):
        return self.at.dev(*self.natural(a, b))

    def exists(self, a, b):
        a, b = self.natural(a, b)
        return 4 * a + b < self.owners

    def block(self, k, a, b, core=None):
        a, b = self.natural(a, b)
        core = self.at.c if core is None else core
        return self.buf.at[k, core * 16 + 4 * a + b, pl.ds(2 * self.way, 2)]

    def half(self, k, a, b, h):
        a, b = self.natural(a, b)
        return self.buf.at[k, self.at.c * 16 + 4 * a + b, pl.ds(2 * self.way + h, 1)]

    def across(self, k, a, b, j, m):
        block = self.block(k, a, b)
        send(block, block, self.sd.at[k, self.way, j, m], self.rd.at[k, self.way, j, m], self.at.partner())

    def first_start(self, k):
        @pl.when(self.exists(self.a, self.b))
        def _():
            own = self.block(k, self.a, self.b)
            for role, by in ((0, 1), (1, -1)):
                send(own, own, self.s1.at[k, self.way, role], self.r1.at[k, self.way, role], self.dev(around(self.a, by), self.b))

    def first_forward(self, k):
        for role, by in ((0, -1), (1, 1)):
            a = around(self.a, by)

            @pl.when(self.exists(a, self.b))
            def _():
                arrived(self.block(k, a, self.b), self.r1.at[k, self.way, role])
                part = self.half(k, a, self.b, role)
                send(
                    part,
                    part,
                    self.s1.at[k, self.way, 2 + role],
                    self.r1.at[k, self.way, 2 + role],
                    self.dev(around(self.a, -by), self.b),
                )

    def first_end(self, k):
        a = around(self.a, 2)

        @pl.when(self.exists(a, self.b))
        def _():
            for role in (0, 1):
                arrived(self.half(k, a, self.b, role), self.r1.at[k, self.way, 2 + role])

    def second_start(self, k, j):
        a = around(self.a, self.offsets[j])

        @pl.when(self.exists(a, self.b))
        def _():
            own = self.block(k, a, self.b)
            for role, by in ((0, 1), (1, -1)):
                send(
                    own, own, self.s2.at[k, self.way, j, role], self.r2.at[k, self.way, j, role], self.dev(self.a, around(self.b, by))
                )
            self.across(k, a, self.b, j, 0)

    def second_forward(self, k, j):
        a = around(self.a, self.offsets[j])
        for role, by in ((0, -1), (1, 1)):
            b = around(self.b, by)

            @pl.when(self.exists(a, b))
            def _():
                arrived(self.block(k, a, b), self.r2.at[k, self.way, j, role])
                part = self.half(k, a, b, role)
                send(
                    part,
                    part,
                    self.s2.at[k, self.way, j, 2 + role],
                    self.r2.at[k, self.way, j, 2 + role],
                    self.dev(self.a, around(self.b, -by)),
                )
                self.across(k, a, b, j, 1 + role)

    def second_end(self, k, j):
        a = around(self.a, self.offsets[j])
        b = around(self.b, 2)

        @pl.when(self.exists(a, b))
        def _():
            for role in (0, 1):
                arrived(self.half(k, a, b, role), self.r2.at[k, self.way, j, 2 + role])
            self.across(k, a, b, j, 3)

    def other_core(self, k):
        for j in range(4):
            a = around(self.b, self.offsets[j])
            for m in range(4):
                b = around(self.a, self.offsets[m])

                @pl.when(self.exists(a, b))
                def _():
                    arrived(self.block(k, a, b, 1 - self.at.c), self.rd.at[k, self.way, j, m])

    def all_sent(self, k):
        own = self.block(k, 0, 0)
        part = self.half(k, 0, 0, 0)

        @pl.when(self.exists(self.a, self.b))
        def _():
            arrived(own, self.s1.at[k, self.way, 0])
            arrived(own, self.s1.at[k, self.way, 1])

        for role, by in ((0, -1), (1, 1)):

            @pl.when(self.exists(around(self.a, by), self.b))
            def _():
                arrived(part, self.s1.at[k, self.way, 2 + role])

        for j in range(4):
            a = around(self.a, self.offsets[j])

            @pl.when(self.exists(a, self.b))
            def _():
                arrived(own, self.s2.at[k, self.way, j, 0])
                arrived(own, self.s2.at[k, self.way, j, 1])
                arrived(own, self.sd.at[k, self.way, j, 0])

            for role, by in ((0, -1), (1, 1)):

                @pl.when(self.exists(a, around(self.b, by)))
                def _():
                    arrived(part, self.s2.at[k, self.way, j, 2 + role])
                    arrived(own, self.sd.at[k, self.way, j, 1 + role])

            @pl.when(self.exists(a, around(self.b, 2)))
            def _():
                arrived(own, self.sd.at[k, self.way, j, 3])


class BothWays:
    def __init__(self, at, buf, owners, sems):
        self.ways = [PlaneGather(at, buf, owners, way, sems) for way in range(2)]

    def __getattr__(self, name):
        def call(*args):
            for way in self.ways:
                getattr(way, name)(*args)

        return call


def swapped(values):
    lane = lax.broadcasted_iota(jnp.int32, values.shape, 1)
    return jnp.where(lax.rem(lane, 32) < 16, pltpu.roll(values, 112, 1), pltpu.roll(values, 16, 1))


def low_norm(values, gain):
    scale = lax.rsqrt(jnp.mean(values * values, axis=-1, keepdims=True) + EPS)
    return (values * scale * gain).astype(jnp.bfloat16)


def main_kernel(
    latent_ref,
    context_ref,
    cond_ref,
    cond_ctx_ref,
    w_mod_ref,
    g_norm_ref,
    w_dq_ref,
    w_dkv_ref,
    w_kr_ref,
    g_cq_ref,
    g_ckv_ref,
    lift_ref,
    row_cos_ref,
    row_sin_ref,
    col_cos_ref,
    col_sin_ref,
    w_uq_hbm,
    w_ukv_hbm,
    w_out_hbm,
    out_ref,
    latent,
    mod_part,
    mod_in,
    mod_mine,
    mod_all,
    x_all,
    h_all,
    w_down,
    compressed,
    item,
    w_uq,
    w_up,
    w_uvt,
    w_out,
    query,
    keys,
    peak,
    total,
    accum,
    w_other,
    heads,
    heads_in,
    pieces,
    pieces_in,
    sums,
    sums_in,
    ms,
    mr,
    as_,
    ar,
    vs,
    vr,
    zs,
    zr,
    *rest,
):
    down_sems, cq_sems, key_sems = rest[0:6], rest[6:12], rest[12:18]
    ws, wr, hs, hr, ps, pr, xs, xr, l1, l2, l3 = rest[18:]
    at = Place()
    owner = exists(at.a, at.b)
    own_slot = at.c * 16 + 4 * at.a + at.b
    own_item = jnp.minimum(at.c * OWNERS + 4 * at.a + at.b, 25)
    in_context = own_item >= 24

    barrier = pltpu.get_barrier_semaphore()

    def greet_z(i, carry):
        pl.semaphore_signal(barrier, inc=1, device_id=(lax.rem(at.z + i, SP), at.t), device_id_type=MESH)
        return carry

    def greet_plane(i, carry):
        pl.semaphore_signal(barrier, inc=1, device_id=(at.z, lax.rem(at.t + i, 32)), device_id_type=MESH)
        return carry

    lax.fori_loop(1, SP, greet_z, 0)
    lax.fori_loop(1, 32, greet_plane, 0)

    loads = [
        pltpu.make_async_copy(w_uq_hbm, w_uq, l1),
        pltpu.make_async_copy(w_ukv_hbm, w_up, l2),
        pltpu.make_async_copy(w_out_hbm, w_out, l3),
    ]
    for load in loads:
        load.start()

    for n in range(4):
        rows = pl.ds(n * 16, 16)
        w_down[0, own_slot, n, :, 0:512] = w_dq_ref[rows, :]
        w_down[0, own_slot, n, :, 512:1024] = w_dkv_ref[rows, :]
        w_down[0, own_slot, n, :, 1024:1152] = jnp.concatenate(
            [w_kr_ref[rows, :], jnp.zeros((16, 64), jnp.bfloat16)], axis=1
        )
    latent[...] = jnp.transpose(latent_ref[...].astype(jnp.float32)).astype(jnp.bfloat16)
    signal = jnp.concatenate([cond_ref[...], cond_ctx_ref[...], jnp.zeros((6, 128), jnp.bfloat16)], axis=0)
    signal = jax.nn.silu(signal.astype(jnp.float32)).astype(jnp.bfloat16)
    partial_mod = nt(signal, w_mod_ref[...])
    mod_part[:, 0:192] = partial_mod[0:1]
    mod_part[:, 192:384] = partial_mod[1:2]
    mod_mine[...] = jnp.zeros(mod_mine.shape, jnp.float32)
    peak[...] = jnp.full(peak.shape, -1e30, jnp.float32)
    total[...] = jnp.zeros(total.shape, jnp.float32)
    accum[...] = jnp.zeros(accum.shape, jnp.float32)

    pl.semaphore_wait(barrier, 46)

    for n in range(1, SP):
        send(mod_part, mod_in.at[n - 1], ms, mr, (lax.rem(at.z - REL[n] + SP, SP), at.t))

    down = BothWays(at, w_down, 16, down_sems)
    down.first_start(0)
    down.second_start(0, 0)

    def give(i, source):
        c = lax.div(i, OWNERS)
        l = i - c * OWNERS
        a, b = lax.div(l, 4), lax.rem(l, 4)
        t = 2 * ((4 * b + a) * (1 - c) + (4 * a + b) * c) + c

        @pl.when(t != at.t)
        def _():
            send(source, x_all.at[own_slot], as_, ar, (at.z, t))

        @pl.when(t == at.t)
        def _():
            x_all[own_slot] = source[...]

    def give_latent(i, carry):
        give(i, latent.at[pl.ds(pl.multiple_of(i * BLOCK, BLOCK), BLOCK)])
        return carry

    lax.fori_loop(0, 24, give_latent, 0)
    for i in (24, 25):
        give(jnp.int32(i), context_ref.at[pl.ds((i - 24) * BLOCK, BLOCK)])

    down.first_forward(0)
    down.second_start(0, 1)
    down.second_start(0, 2)
    loads[1].wait()
    w_uvt[...] = jnp.transpose(w_up[:, NOPE:].astype(jnp.float32)).astype(jnp.bfloat16)
    down.first_end(0)
    down.second_start(0, 3)

    arrived(mod_in, mr)
    mod = mod_part[...]
    for n in range(SP - 1):
        mod = mod + mod_in[n]
    mod_mine[:, 0:384] = mod
    mod_mine[:, 384:448] = g_norm_ref[...]
    mod_all[own_slot] = mod_mine[...]

    def tell(i, carry):
        send(mod_mine, mod_all.at[own_slot], vs, vr, (at.z, lax.rem(at.t + i, 32)))
        return carry

    lax.fori_loop(1, 32, tell, 0)

    for j in range(4):
        down.second_forward(0, j)

    @pl.when(owner)
    def _():
        arrived(x_all.at[pl.ds(0, 31)], ar)

    x = x_all[...].astype(jnp.float32)
    squares = jnp.sum(jnp.sum(x * x, axis=0), axis=1, keepdims=True)
    norm = lax.rsqrt(squares / D + EPS)
    for j in range(4):
        down.second_end(0, j)
    loads[2].wait()
    send(w_out, w_other, ws, wr, at.partner())
    arrived(mod_all.at[pl.ds(0, 31)], vr)
    for s in range(0, 32, 2):
        pair = []
        for slot in (s, s + 1):
            m = mod_all[slot]
            shift = jnp.where(in_context, m[:, 192:256], m[:, 0:64])
            scale = jnp.where(in_context, m[:, 256:320], m[:, 64:128])
            pair.append((x[slot] * norm * m[:, 384:448] * (1.0 + scale) + shift).astype(jnp.bfloat16))
        h_all[:, s * 64 : s * 64 + 128] = jnp.concatenate(pair, axis=1)
    down.other_core(0)
    low = nn(h_all[...], w_down[0].reshape(D, 1152))

    first_row = at.z * 6
    item_row = first_row + lax.div(jnp.minimum(own_item, 23), 4)
    item_col = pl.ds(pl.multiple_of(lax.rem(own_item, 4) * BLOCK, BLOCK), BLOCK)
    item_cos = jnp.where(in_context, 1.0, row_cos_ref[pl.ds(item_row, 1), :] + col_cos_ref[item_col, :])
    item_sin = jnp.where(in_context, 0.0, row_sin_ref[pl.ds(item_row, 1), :] + col_sin_ref[item_col, :])
    rotary = low[:, 1024:1152]
    rotary = rotary * item_cos + swapped(rotary) * item_sin
    item[:, 0:512] = low_norm(low[:, 512:1024], g_ckv_ref[...])
    item[:, 512:640] = rotary.astype(jnp.bfloat16)
    cq = low_norm(low[:, 0:512], g_cq_ref[...])
    for n in range(4):
        compressed[0, own_slot, n] = cq[:, 128 * n : 128 * n + 128]

    @pl.when(owner)
    def _():
        keys[0, own_slot, 0] = item[...]
        for n in range(1, SP):
            k, i = divmod(n, 4)
            send(
                item,
                keys.at[k, own_slot, i],
                zs.at[k],
                zr.at[k],
                (lax.rem(at.z - REL[n] + SP, SP), at.t),
            )

    ask = BothWays(at, compressed, OWNERS, cq_sems)
    gather = BothWays(at, keys, OWNERS, key_sems)
    ask.first_start(0)
    ask.second_start(0, 0)

    def chunk_here(k):
        @pl.when(owner)
        def _():
            arrived(keys.at[k, own_slot], zr.at[k])

    lift = lift_ref[0, 0] * LOG2E

    def attend(k, g):
        block = keys[k, pl.ds(g * 16, OWNERS)].reshape(OWNERS * 4 * BLOCK, 640)
        ckv = block[:, :512]
        key = jnp.concatenate([nn(ckv, w_up[:, :NOPE]).astype(jnp.bfloat16), block[:, 512:]], axis=1)
        value = nt(w_uvt[...], ckv).astype(jnp.bfloat16)
        score = nt(key, query[...]) * (SCALE * LOG2E)
        extra = jnp.where(g == 1, lift, 0.0)
        score = jnp.concatenate([score[: 11 * 4 * BLOCK], score[11 * 4 * BLOCK :] + extra], axis=0)
        fresh = jnp.maximum(peak[...], jnp.max(score, axis=0, keepdims=True))
        probs = jnp.exp2(score - fresh)
        fade = jnp.exp2(peak[...] - fresh)
        peak[...] = fresh
        total[...] = total[...] * fade + jnp.sum(probs, axis=0, keepdims=True)
        accum[...] = accum[...] * fade + nn(value, probs.astype(jnp.bfloat16))

    @pl.when(owner)
    def _():
        arrived(keys.at[0, own_slot, pl.ds(1, 3)], zr.at[0])

    gather.first_start(0)
    gather.second_start(0, 0)
    ask.first_forward(0)
    ask.second_start(0, 1)
    ask.second_start(0, 2)
    gather.first_forward(0)
    gather.second_start(0, 1)
    gather.second_start(0, 2)
    ask.first_end(0)
    ask.second_start(0, 3)
    gather.first_end(0)
    gather.second_start(0, 3)
    chunk_here(1)
    gather.first_start(1)
    for j in range(4):
        ask.second_forward(0, j)
    for j in range(4):
        ask.second_end(0, j)

    def make_query():
        loads[0].wait()
        ask.other_core(0)
        cq = jnp.concatenate(
            [
                jnp.concatenate([compressed[0, pl.ds(16 * c, 13 - 2 * c), n].reshape(-1, 128) for n in range(4)], axis=1)
                for c in range(2)
            ],
            axis=0,
        )
        query[:, 0:NOPE] = nt(cq, w_uq[0:NOPE, :]).astype(jnp.bfloat16)
        turn = nt(cq, w_uq[NOPE:, :])
        turn = jnp.concatenate([turn, jnp.zeros_like(turn)], axis=1)
        for r in range(6):
            values = turn[64 * r : 64 * r + 64]
            cosine = row_cos_ref[pl.ds(first_row + r, 1), :] + col_cos_ref[...]
            sine = row_sin_ref[pl.ds(first_row + r, 1), :] + col_sin_ref[...]
            query[64 * r : 64 * r + 64, NOPE:] = (values * cosine + swapped(values) * sine).astype(jnp.bfloat16)

    def step(k, carry):
        @pl.when(k < CHUNKS)
        def _():
            gather.second_forward(k, 0)
            gather.second_forward(k, 1)

        @pl.when(k == 0)
        def _():
            make_query()

        @pl.when(k > 0)
        def _():
            attend(k - 1, at.c)

        @pl.when(k < CHUNKS - 1)
        def _():
            gather.first_forward(k + 1)
            gather.second_start(k + 1, 0)
            gather.second_start(k + 1, 1)
            gather.second_start(k + 1, 2)

        @pl.when(k < CHUNKS)
        def _():
            gather.second_forward(k, 2)
            gather.second_forward(k, 3)

        @pl.when(k < CHUNKS - 1)
        def _():
            gather.first_end(k + 1)
            gather.second_start(k + 1, 3)

        @pl.when(k < CHUNKS - 2)
        def _():
            chunk_here(k + 2)
            gather.first_start(k + 2)

        @pl.when(k > 0)
        def _():
            gather.other_core(k - 1)
            attend(k - 1, 1 - at.c)

        @pl.when(k < CHUNKS)
        def _():
            for j in range(4):
                gather.second_end(k, j)

        return carry

    lax.fori_loop(0, CHUNKS + 1, step, 0)

    rows = heads_in.shape[0]
    heads[...] = jnp.transpose(accum[...] / total[...]).astype(jnp.bfloat16)
    theirs = heads.at[pl.ds((1 - at.c) * rows, rows)]
    send(theirs, heads_in, hs, hr, at.partner())
    arrived(w_other, wr)
    arrived(heads_in, hr)
    mine = heads[pl.ds(at.c * rows, rows), :]
    other = heads_in[...]

    def product(p):
        columns = pl.ds(pl.multiple_of(p * 128, 128), 128)
        return nn(mine, w_out[:, columns]) + nn(other, w_other[:, columns])

    for n, (dy, dx) in enumerate(FAR_FIRST):
        p = 4 * around(at.y, dy) + around(at.x, dx)
        pieces[n] = product(p).astype(jnp.bfloat16)
        send(pieces.at[n], pieces_in.at[n], ps, pr, (at.z, 2 * p + at.c))
    here = product(at.p)
    arrived(pieces_in, pr)
    for n in range(15):
        here = here + pieces_in[n].astype(jnp.float32)
    sums[...] = here
    send(sums, sums_in, xs, xr, at.partner())
    gate = mod_mine[:, 128:192]

    def columns_here(value):
        return gate * jnp.where(at.c == 0, value[:, :64], value[:, 64:])

    here = columns_here(here)
    arrived(sums_in, xr)
    there = columns_here(sums_in[...])
    branch = jnp.concatenate([jnp.where(at.c == 0, here, there), jnp.where(at.c == 0, there, here)], axis=0)
    out_ref[...] = (latent_ref[...].astype(jnp.float32) + jnp.transpose(branch)).astype(jnp.bfloat16)

    arrived(mod_in, ms)
    arrived(mod_all.at[pl.ds(0, 31)], vs)
    arrived(w_other, ws)
    arrived(heads_in, hs)
    arrived(pieces_in, ps)
    arrived(sums_in, xs)

    @pl.when(owner)
    def _():
        arrived(x_all.at[pl.ds(0, 25)], as_)
        arrived(keys.at[0, 0, pl.ds(1, 3)], zs.at[0])
        for k in range(1, CHUNKS):
            arrived(keys.at[k, 0], zs.at[k])

    @pl.when(jnp.logical_not(owner))
    def _():
        arrived(x_all.at[pl.ds(0, 26)], as_)

    down.all_sent(0)
    ask.all_sent(0)

    def sent(k, carry):
        gather.all_sent(k)
        return carry

    lax.fori_loop(0, CHUNKS, sent, 0)


def gather_sems(chunks):
    dma = pltpu.SemaphoreType.DMA
    few, many = dma((chunks, 2, 4)), dma((chunks, 2, 4, 4))
    return [few, few, many, many, many, many]


def turn_tables():
    half = ROPE // 2
    inverse = (np.float32(1.0) / np.float32(THETA) ** (np.arange(0, half, 2, dtype=np.float32) / np.float32(half))).astype(
        np.float32
    )

    def table(count, start):
        angle = (np.arange(count, dtype=np.float32)[:, None] * inverse).astype(np.float32)
        cosine, sine = np.cos(angle), np.sin(angle)
        whole_cos = np.zeros((count, 128), np.float32)
        whole_sin = np.zeros((count, 128), np.float32)
        whole_cos[:, start : start + 32] = np.concatenate([cosine, cosine], axis=1)
        whole_sin[:, start : start + 32] = np.concatenate([-sine, sine], axis=1)
        return whole_cos, whole_sin

    return table(6144 // GRID_W, 0) + table(GRID_W, 32)


def per_device(
    latent, context, cond, cond_ctx, w_mod, g_norm, w_dq, w_dkv, w_kr, g_cq, g_ckv, w_uq, w_ukv, ctx_lift, w_out
):
    rows = latent.shape[0]
    vmem = pl.BlockSpec(memory_space=pltpu.VMEM)
    smem = pl.BlockSpec(memory_space=pltpu.SMEM)
    hbm = pl.BlockSpec(memory_space=pltpu.HBM)
    dma = pltpu.SemaphoreType.DMA
    bf16, f32 = jnp.bfloat16, jnp.float32
    return pl.pallas_call(
        main_kernel,
        out_shape=jax.ShapeDtypeStruct((64, rows), bf16),
        in_specs=[vmem] * 11 + [smem] + [vmem] * 4 + [hbm] * 3,
        out_specs=vmem,
        scratch_shapes=[
            pltpu.VMEM((rows, 64), bf16),
            pltpu.VMEM((1, 384), f32),
            pltpu.VMEM((SP - 1, 1, 384), f32),
            pltpu.VMEM((1, 512), f32),
            pltpu.VMEM((32, 1, 512), f32),
            pltpu.VMEM((32, BLOCK, 64), bf16),
            pltpu.VMEM((BLOCK, D), bf16),
            pltpu.VMEM((1, 32, 4, 16, 1152), bf16),
            pltpu.VMEM((1, 32, 4, BLOCK, 128), bf16),
            pltpu.VMEM((BLOCK, 640), bf16),
            pltpu.VMEM((NOPE + ROPE, 512), bf16),
            pltpu.VMEM((512, NOPE + DV), bf16),
            pltpu.VMEM((DV, 512), bf16),
            pltpu.VMEM((DV, D), bf16),
            pltpu.VMEM((rows, 256), bf16),
            pltpu.VMEM((CHUNKS, 32, 4, BLOCK, 640), bf16),
            pltpu.VMEM((1, rows), f32),
            pltpu.VMEM((1, rows), f32),
            pltpu.VMEM((DV, rows), f32),
            pltpu.VMEM((DV, D), bf16),
            pltpu.VMEM((rows, DV), bf16),
            pltpu.VMEM((rows // 2, DV), bf16),
            pltpu.VMEM((15, rows // 2, 128), bf16),
            pltpu.VMEM((15, rows // 2, 128), bf16),
            pltpu.VMEM((rows // 2, 128), f32),
            pltpu.VMEM((rows // 2, 128), f32),
            dma,
            dma,
            dma,
            dma,
            dma,
            dma,
            dma((CHUNKS,)),
            dma((CHUNKS,)),
            *gather_sems(1),
            *gather_sems(1),
            *gather_sems(CHUNKS),
            *[dma] * 11,
        ],
        compiler_params=pltpu.CompilerParams(
            collective_id=0, has_side_effects=True, vmem_limit_bytes=56 * 1024 * 1024
        ),
        name="main",
    )(
        latent.T,
        context,
        cond[None, :],
        cond_ctx[None, :],
        jnp.transpose(w_mod, (1, 2, 0)).reshape(192, 128),
        g_norm[None, :],
        w_dq,
        w_dkv,
        w_kr,
        g_cq[None, :],
        g_ckv[None, :],
        ctx_lift.reshape(1, 1),
        *turn_tables(),
        w_uq[:, 0, :].T,
        w_ukv[:, 0, :],
        w_out[0],
    ).T


def solution(mesh):
    return jax.shard_map(
        per_device,
        mesh=mesh,
        in_specs=(
            P("sp", "tp"),
            P("sp", "tp"),
            P("sp"),
            P("sp"),
            P("sp", None, "tp"),
            P("tp"),
            P("tp", None),
            P("tp", None),
            P("tp", None),
            P(),
            P(),
            P(None, "tp", None),
            P(None, "tp", None),
            P("tp"),
            P("tp", None, None),
        ),
        out_specs=P("sp", "tp"),
        check_vma=False,
    )
```

```python
import numpy as np

import jax
import jax.numpy as jnp
from jax import lax
from jax.experimental import pallas as pl
from jax.experimental.pallas import tpu as pltpu

from jax.sharding import PartitionSpec as P

MESH = pl.DeviceIdType.MESH
D = 2048
NOPE = 128
ROPE = 64
DV = 128
GRID_W = 64
EPS = 1e-06
THETA = 10000.0
LOG2E = 1.4426950408889634
SCALE = (NOPE + ROPE) ** (-0.5)

BLOCK = 16
OWNERS = 13
SP = 16
CHUNKS = 4
REL = (0, 1, -1, 2, -2, 3, -3, 4, -4, 5, -5, 6, -6, 7, -7, 8)
FAR_FIRST = tuple(
    sorted(
        [(dy, dx) for dy in range(4) for dx in range(4) if dy or dx],
        key=lambda o: -(min(o[0], 4 - o[0]) + min(o[1], 4 - o[1])),
    )
)


def nn(lhs, rhs):
    return jnp.dot(lhs, rhs, preferred_element_type=jnp.float32)


def nt(lhs, rhs):
    return lax.dot_general(lhs, rhs, (((1,), (1,)), ((), ())), preferred_element_type=jnp.float32)


class Place:
    def __init__(self):
        self.z = lax.axis_index("sp")
        self.t = lax.axis_index("tp")
        self.p = lax.div(self.t, 2)
        self.c = lax.rem(self.t, 2)
        self.y = lax.div(self.p, 4)
        self.x = lax.rem(self.p, 4)
        self.a = self.x * (1 - self.c) + self.y * self.c
        self.b = self.y * (1 - self.c) + self.x * self.c

    def dev(self, a, b):
        p = (4 * b + a) * (1 - self.c) + (4 * a + b) * self.c
        return (self.z, 2 * p + self.c)

    def partner(self):
        return (self.z, 2 * self.p + 1 - self.c)


def around(i, by):
    return lax.rem(i + by + 4, 4)


def exists(a, b):
    return 4 * a + b < OWNERS


def send(src, dst, send_sem, recv_sem, device):
    copy = pltpu.make_async_remote_copy(
        src_ref=src,
        dst_ref=dst,
        send_sem=send_sem,
        recv_sem=recv_sem,
        device_id=device,
        device_id_type=MESH,
    )
    copy.start()


def arrived(ref, sem):
    pltpu.make_async_copy(ref, ref, sem).wait()


class PlaneGather:
    def __init__(self, at, buf, owners, way, sems):
        self.size = buf.shape[2] // 2
        self.at = at
        self.buf = buf
        self.owners = owners
        self.way = way
        self.s1, self.r1, self.s2, self.r2, self.sd, self.rd = sems
        self.offsets = (0, -1, 1, 2)
        self.a, self.b = (at.a, at.b) if way == 0 else (at.b, at.a)

    def natural(self, a, b):
        return (a, b) if self.way == 0 else (b, a)

    def dev(self, a, b):
        return self.at.dev(*self.natural(a, b))

    def exists(self, a, b):
        a, b = self.natural(a, b)
        return 4 * a + b < self.owners

    def block(self, k, a, b, core=None):
        a, b = self.natural(a, b)
        core = self.at.c if core is None else core
        return self.buf.at[k, core * 16 + 4 * a + b, pl.ds(self.size * self.way, self.size)]

    def across(self, k, a, b, j, m):
        block = self.block(k, a, b)
        send(block, block, self.sd.at[k, self.way, j, m], self.rd.at[k, self.way, j, m], self.at.partner())

    def first_start(self, k):
        @pl.when(self.exists(self.a, self.b))
        def _():
            own = self.block(k, self.a, self.b)
            for role, by in ((0, 1), (1, -1)):
                send(own, own, self.s1.at[k, self.way, role], self.r1.at[k, self.way, role], self.dev(around(self.a, by), self.b))

    def first_forward(self, k):
        for role, by in ((0, -1), (1, 1)):
            a = around(self.a, by)

            @pl.when(self.exists(a, self.b))
            def _():
                block = self.block(k, a, self.b)
                arrived(block, self.r1.at[k, self.way, role])
                if role == self.way:
                    send(block, block, self.s1.at[k, self.way, 2], self.r1.at[k, self.way, 2], self.dev(around(self.a, -by), self.b))

    def first_end(self, k):
        a = around(self.a, 2)

        @pl.when(self.exists(a, self.b))
        def _():
            arrived(self.block(k, a, self.b), self.r1.at[k, self.way, 2])

    def second_start(self, k, j):
        a = around(self.a, self.offsets[j])

        @pl.when(self.exists(a, self.b))
        def _():
            own = self.block(k, a, self.b)
            for role, by in ((0, 1), (1, -1)):
                send(
                    own, own, self.s2.at[k, self.way, j, role], self.r2.at[k, self.way, j, role], self.dev(self.a, around(self.b, by))
                )
            self.across(k, a, self.b, j, 0)

    def second_forward(self, k, j):
        a = around(self.a, self.offsets[j])
        for role, by in ((0, -1), (1, 1)):
            b = around(self.b, by)

            @pl.when(self.exists(a, b))
            def _():
                block = self.block(k, a, b)
                arrived(block, self.r2.at[k, self.way, j, role])
                if role == j % 2:
                    send(
                        block,
                        block,
                        self.s2.at[k, self.way, j, 2],
                        self.r2.at[k, self.way, j, 2],
                        self.dev(self.a, around(self.b, -by)),
                    )
                self.across(k, a, b, j, 1 + role)

    def second_end(self, k, j):
        a = around(self.a, self.offsets[j])
        b = around(self.b, 2)

        @pl.when(self.exists(a, b))
        def _():
            arrived(self.block(k, a, b), self.r2.at[k, self.way, j, 2])
            self.across(k, a, b, j, 3)

    def other_core(self, k):
        for j in range(4):
            a = around(self.b, self.offsets[j])
            for m in range(4):
                b = around(self.a, self.offsets[m])

                @pl.when(self.exists(a, b))
                def _():
                    arrived(self.block(k, a, b, 1 - self.at.c), self.rd.at[k, self.way, j, m])

    def all_sent(self, k):
        own = self.block(k, 0, 0)

        @pl.when(self.exists(self.a, self.b))
        def _():
            arrived(own, self.s1.at[k, self.way, 0])
            arrived(own, self.s1.at[k, self.way, 1])

        @pl.when(self.exists(around(self.a, 1 if self.way else -1), self.b))
        def _():
            arrived(own, self.s1.at[k, self.way, 2])

        for j in range(4):
            a = around(self.a, self.offsets[j])

            @pl.when(self.exists(a, self.b))
            def _():
                arrived(own, self.s2.at[k, self.way, j, 0])
                arrived(own, self.s2.at[k, self.way, j, 1])
                arrived(own, self.sd.at[k, self.way, j, 0])

            for role, by in ((0, -1), (1, 1)):

                @pl.when(self.exists(a, around(self.b, by)))
                def _():
                    if role == j % 2:
                        arrived(own, self.s2.at[k, self.way, j, 2])
                    arrived(own, self.sd.at[k, self.way, j, 1 + role])

            @pl.when(self.exists(a, around(self.b, 2)))
            def _():
                arrived(own, self.sd.at[k, self.way, j, 3])


class BothWays:
    def __init__(self, at, buf, owners, sems):
        self.ways = [PlaneGather(at, buf, owners, way, sems) for way in range(2)]

    def __getattr__(self, name):
        def call(*args):
            for way in self.ways:
                getattr(way, name)(*args)

        return call


def swapped(values):
    lane = lax.broadcasted_iota(jnp.int32, values.shape, 1)
    return jnp.where(lax.rem(lane, 32) < 16, pltpu.roll(values, 112, 1), pltpu.roll(values, 16, 1))


def low_norm(values, gain):
    scale = lax.rsqrt(jnp.mean(values * values, axis=-1, keepdims=True) + EPS)
    return (values * scale * gain).astype(jnp.bfloat16)


def main_kernel(
    latent_ref,
    context_ref,
    cond_ref,
    cond_ctx_ref,
    w_mod_ref,
    g_norm_ref,
    w_dq_ref,
    w_dkv_ref,
    w_kr_ref,
    g_cq_ref,
    g_ckv_ref,
    lift_ref,
    row_cos_ref,
    row_sin_ref,
    col_cos_ref,
    col_sin_ref,
    w_uq_hbm,
    w_ukv_hbm,
    w_out_hbm,
    out_ref,
    latent,
    mod_part,
    mod_in,
    mod_mine,
    mod_all,
    x_all,
    h_all,
    w_down,
    compressed,
    item,
    turned,
    turned_in,
    w_uq,
    w_up,
    w_uvt,
    w_out,
    query,
    keys,
    peak,
    total,
    accum,
    w_other,
    heads,
    heads_in,
    pieces,
    pieces_in,
    sums,
    sums_in,
    ms,
    mr,
    as_,
    ar,
    vs,
    vr,
    zs,
    zr,
    ts,
    tr,
    *rest,
):
    down_sems, cq_sems, key_sems = rest[0:6], rest[6:12], rest[12:18]
    ws, wr, hs, hr, ps, pr, xs, xr, l1, l2, l3 = rest[18:]
    at = Place()
    owner = exists(at.a, at.b)
    own_slot = at.c * 16 + 4 * at.a + at.b
    own_item = jnp.minimum(at.c * OWNERS + 4 * at.a + at.b, 25)
    in_context = own_item >= 24

    barrier = pltpu.get_barrier_semaphore()

    def greet_z(i, carry):
        pl.semaphore_signal(barrier, inc=1, device_id=(lax.rem(at.z + i, SP), at.t), device_id_type=MESH)
        return carry

    def greet_plane(i, carry):
        pl.semaphore_signal(barrier, inc=1, device_id=(at.z, lax.rem(at.t + i, 32)), device_id_type=MESH)
        return carry

    lax.fori_loop(1, SP, greet_z, 0)
    lax.fori_loop(1, 32, greet_plane, 0)

    loads = [
        pltpu.make_async_copy(w_uq_hbm, w_uq, l1),
        pltpu.make_async_copy(w_ukv_hbm, w_up, l2),
        pltpu.make_async_copy(w_out_hbm, w_out, l3),
    ]
    for load in loads:
        load.start()

    for n in range(4):
        rows = pl.ds(n * 16, 16)
        w_down[0, own_slot, n, :, 0:512] = w_dq_ref[rows, :]
        w_down[0, own_slot, n, :, 512:1024] = w_dkv_ref[rows, :]
        w_down[0, own_slot, n, :, 1024:1152] = jnp.concatenate(
            [w_kr_ref[rows, :], jnp.zeros((16, 64), jnp.bfloat16)], axis=1
        )
    latent[...] = jnp.transpose(latent_ref[...].astype(jnp.float32)).astype(jnp.bfloat16)
    signal = jnp.concatenate([cond_ref[...], cond_ctx_ref[...], jnp.zeros((6, 128), jnp.bfloat16)], axis=0)
    signal = jax.nn.silu(signal.astype(jnp.float32)).astype(jnp.bfloat16)
    partial_mod = nt(signal, w_mod_ref[...])
    mod_part[:, 0:192] = partial_mod[0:1]
    mod_part[:, 192:384] = partial_mod[1:2]
    mod_mine[...] = jnp.zeros(mod_mine.shape, jnp.float32)
    peak[...] = jnp.full(peak.shape, -1e30, jnp.float32)
    total[...] = jnp.zeros(total.shape, jnp.float32)
    accum[...] = jnp.zeros(accum.shape, jnp.float32)

    pl.semaphore_wait(barrier, 46)

    for n in range(1, SP):
        send(mod_part, mod_in.at[n - 1], ms, mr, (lax.rem(at.z - REL[n] + SP, SP), at.t))

    down = BothWays(at, w_down, 16, down_sems)
    down.first_start(0)
    down.second_start(0, 0)

    def give(i, source):
        c = lax.div(i, OWNERS)
        l = i - c * OWNERS
        a, b = lax.div(l, 4), lax.rem(l, 4)
        t = 2 * ((4 * b + a) * (1 - c) + (4 * a + b) * c) + c

        @pl.when(t != at.t)
        def _():
            send(source, x_all.at[own_slot], as_, ar, (at.z, t))

        @pl.when(t == at.t)
        def _():
            x_all[own_slot] = source[...]

    def give_latent(i, carry):
        give(i, latent.at[pl.ds(pl.multiple_of(i * BLOCK, BLOCK), BLOCK)])
        return carry

    lax.fori_loop(0, 24, give_latent, 0)
    for i in (24, 25):
        give(jnp.int32(i), context_ref.at[pl.ds((i - 24) * BLOCK, BLOCK)])

    down.first_forward(0)
    down.second_start(0, 1)
    down.second_start(0, 2)
    loads[1].wait()
    w_uvt[...] = jnp.transpose(w_up[:, NOPE:].astype(jnp.float32)).astype(jnp.bfloat16)
    down.first_end(0)
    down.second_start(0, 3)

    arrived(mod_in, mr)
    mod = mod_part[...]
    for n in range(SP - 1):
        mod = mod + mod_in[n]
    mod_mine[:, 0:384] = mod
    mod_mine[:, 384:448] = g_norm_ref[...]
    mod_all[own_slot] = mod_mine[...]

    def tell(i, carry):
        send(mod_mine, mod_all.at[own_slot], vs, vr, (at.z, lax.rem(at.t + i, 32)))
        return carry

    lax.fori_loop(1, 32, tell, 0)

    for j in range(4):
        down.second_forward(0, j)

    @pl.when(owner)
    def _():
        arrived(x_all.at[pl.ds(0, 31)], ar)

    x = x_all[...].astype(jnp.float32)
    squares = jnp.sum(jnp.sum(x * x, axis=0), axis=1, keepdims=True)
    norm = lax.rsqrt(squares / D + EPS)
    for j in range(4):
        down.second_end(0, j)
    loads[2].wait()
    send(w_out, w_other, ws, wr, at.partner())
    arrived(mod_all.at[pl.ds(0, 31)], vr)
    for s in range(0, 32, 2):
        pair = []
        for slot in (s, s + 1):
            m = mod_all[slot]
            shift = jnp.where(in_context, m[:, 192:256], m[:, 0:64])
            scale = jnp.where(in_context, m[:, 256:320], m[:, 64:128])
            pair.append((x[slot] * norm * m[:, 384:448] * (1.0 + scale) + shift).astype(jnp.bfloat16))
        h_all[:, s * 64 : s * 64 + 128] = jnp.concatenate(pair, axis=1)
    down.other_core(0)
    low = nn(h_all[...], w_down[0].reshape(D, 1152))

    first_row = at.z * 6
    item_row = first_row + lax.div(jnp.minimum(own_item, 23), 4)
    item_col = pl.ds(pl.multiple_of(lax.rem(own_item, 4) * BLOCK, BLOCK), BLOCK)
    item_cos = jnp.where(in_context, 1.0, row_cos_ref[pl.ds(item_row, 1), :] + col_cos_ref[item_col, :])
    item_sin = jnp.where(in_context, 0.0, row_sin_ref[pl.ds(item_row, 1), :] + col_sin_ref[item_col, :])
    rotary = low[:, 1024:1152]
    rotary = rotary * item_cos + swapped(rotary) * item_sin
    ckv_own = low_norm(low[:, 512:1024], g_ckv_ref[...])
    for n in range(4):
        item[n] = ckv_own[:, 128 * n : 128 * n + 128]
    turned[...] = (rotary + pltpu.roll(rotary, 64, 1)).astype(jnp.bfloat16)
    cq = low_norm(low[:, 0:512], g_cq_ref[...])
    for n in range(4):
        compressed[0, own_slot, n] = cq[:, 128 * n : 128 * n + 128]

    @pl.when(owner)
    def _():
        keys[0, own_slot, 0:4] = item[...]
        turned_in[0, 0] = turned[...]
        for n in range(1, SP):
            k, i = divmod(n, 4)
            there = (lax.rem(at.z - REL[n] + SP, SP), at.t)
            send(item, keys.at[k, own_slot, pl.ds(9 * (i // 2) + 4 * (i % 2), 4)], zs.at[k], zr.at[k], there)
            send(turned, turned_in.at[k, i], ts.at[k], tr.at[k], there)

    ask = BothWays(at, compressed, OWNERS, cq_sems)
    gather = BothWays(at, keys, OWNERS, key_sems)
    ask.first_start(0)
    ask.second_start(0, 0)

    def join_turned(k):
        for way in range(2):
            first = turned_in[k, 2 * way].astype(jnp.float32)
            second = turned_in[k, 2 * way + 1].astype(jnp.float32)
            lane = lax.broadcasted_iota(jnp.int32, first.shape, 1)
            keys[k, own_slot, 9 * way + 8] = jnp.where(lane < 64, first, second).astype(jnp.bfloat16)

    def chunk_here(k):
        @pl.when(owner)
        def _():
            arrived(keys.at[k, own_slot, pl.ds(0, 16)], zr.at[k])
            arrived(turned_in.at[k], tr.at[k])
            join_turned(k)

    lift = lift_ref[0, 0] * LOG2E

    def attend(k, g):
        slots = pl.ds(g * 16, OWNERS)
        count = OWNERS * BLOCK
        ckv = jnp.concatenate(
            [
                jnp.concatenate([keys[k, slots, 9 * w + 4 * i + n].reshape(count, 128) for n in range(4)], axis=1)
                for w in range(2)
                for i in range(2)
            ],
            axis=0,
        )
        key = nn(ckv, w_up[:, :NOPE]).astype(jnp.bfloat16)
        value = nt(w_uvt[...], ckv).astype(jnp.bfloat16)
        extra = jnp.where(g == 1, lift, 0.0)
        scores = []
        for w in range(2):
            rotary_key = keys[k, slots, 9 * w + 8].reshape(count, 128)
            for i in range(2):
                first = (2 * w + i) * count
                both = jnp.concatenate([key[first : first + count], rotary_key], axis=1)
                part = nt(both, query[i]) * (SCALE * LOG2E)
                scores += [part[: 11 * BLOCK], part[11 * BLOCK :] + extra]
        score = jnp.concatenate(scores, axis=0)
        fresh = jnp.maximum(peak[...], jnp.max(score, axis=0, keepdims=True))
        probs = jnp.exp2(score - fresh)
        fade = jnp.exp2(peak[...] - fresh)
        peak[...] = fresh
        total[...] = total[...] * fade + jnp.sum(probs, axis=0, keepdims=True)
        accum[...] = accum[...] * fade + nn(value, probs.astype(jnp.bfloat16))

    @pl.when(owner)
    def _():
        arrived(keys.at[0, own_slot, pl.ds(0, 12)], zr.at[0])
        arrived(turned_in.at[0, pl.ds(1, 3)], tr.at[0])
        join_turned(0)

    gather.first_start(0)
    gather.second_start(0, 0)
    ask.first_forward(0)
    ask.second_start(0, 1)
    ask.second_start(0, 2)
    gather.first_forward(0)
    gather.second_start(0, 1)
    gather.second_start(0, 2)
    ask.first_end(0)
    ask.second_start(0, 3)
    gather.first_end(0)
    gather.second_start(0, 3)
    chunk_here(1)
    gather.first_start(1)
    for j in range(4):
        ask.second_forward(0, j)
    for j in range(4):
        ask.second_end(0, j)

    def make_query():
        loads[0].wait()
        ask.other_core(0)
        cq = jnp.concatenate(
            [
                jnp.concatenate([compressed[0, pl.ds(16 * c, 13 - 2 * c), n].reshape(-1, 128) for n in range(4)], axis=1)
                for c in range(2)
            ],
            axis=0,
        )
        plain = nt(cq, w_uq[0:NOPE, :]).astype(jnp.bfloat16)
        query[0, :, 0:NOPE] = plain
        query[1, :, 0:NOPE] = plain
        turn = nt(cq, w_uq[NOPE:, :])
        turn = jnp.concatenate([turn, jnp.zeros_like(turn)], axis=1)
        for r in range(6):
            values = turn[64 * r : 64 * r + 64]
            cosine = row_cos_ref[pl.ds(first_row + r, 1), :] + col_cos_ref[...]
            sine = row_sin_ref[pl.ds(first_row + r, 1), :] + col_sin_ref[...]
            values = values * cosine + swapped(values) * sine
            query[0, 64 * r : 64 * r + 64, NOPE:] = values.astype(jnp.bfloat16)
            query[1, 64 * r : 64 * r + 64, NOPE:] = pltpu.roll(values, 64, 1).astype(jnp.bfloat16)

    def step(k, carry):
        @pl.when(k < CHUNKS)
        def _():
            gather.second_forward(k, 0)
            gather.second_forward(k, 1)

        @pl.when(k == 0)
        def _():
            make_query()

        @pl.when(k > 0)
        def _():
            attend(k - 1, at.c)

        @pl.when(k < CHUNKS - 1)
        def _():
            gather.first_forward(k + 1)
            gather.second_start(k + 1, 0)
            gather.second_start(k + 1, 1)
            gather.second_start(k + 1, 2)

        @pl.when(k < CHUNKS)
        def _():
            gather.second_forward(k, 2)
            gather.second_forward(k, 3)

        @pl.when(k < CHUNKS - 1)
        def _():
            gather.first_end(k + 1)
            gather.second_start(k + 1, 3)

        @pl.when(k < CHUNKS - 2)
        def _():
            chunk_here(k + 2)
            gather.first_start(k + 2)

        @pl.when(k > 0)
        def _():
            gather.other_core(k - 1)
            attend(k - 1, 1 - at.c)

        @pl.when(k < CHUNKS)
        def _():
            for j in range(4):
                gather.second_end(k, j)

        return carry

    lax.fori_loop(0, CHUNKS + 1, step, 0)

    rows = heads_in.shape[0]
    heads[...] = jnp.transpose(accum[...] / total[...]).astype(jnp.bfloat16)
    theirs = heads.at[pl.ds((1 - at.c) * rows, rows)]
    send(theirs, heads_in, hs, hr, at.partner())
    arrived(w_other, wr)
    arrived(heads_in, hr)
    mine = heads[pl.ds(at.c * rows, rows), :]
    other = heads_in[...]

    def product(p):
        columns = pl.ds(pl.multiple_of(p * 128, 128), 128)
        return nn(mine, w_out[:, columns]) + nn(other, w_other[:, columns])

    for n, (dy, dx) in enumerate(FAR_FIRST):
        p = 4 * around(at.y, dy) + around(at.x, dx)
        pieces[n] = product(p).astype(jnp.bfloat16)
        send(pieces.at[n], pieces_in.at[n], ps, pr, (at.z, 2 * p + at.c))
    here = product(at.p)
    arrived(mod_in, ms)
    arrived(mod_all.at[pl.ds(0, 31)], vs)
    arrived(w_other, ws)
    arrived(heads_in, hs)

    @pl.when(owner)
    def _():
        arrived(x_all.at[pl.ds(0, 25)], as_)
        arrived(keys.at[0, 0, pl.ds(0, 12)], zs.at[0])
        arrived(turned_in.at[0, pl.ds(1, 3)], ts.at[0])
        for k in range(1, CHUNKS):
            arrived(keys.at[k, 0, pl.ds(0, 16)], zs.at[k])
            arrived(turned_in.at[k], ts.at[k])

    @pl.when(jnp.logical_not(owner))
    def _():
        arrived(x_all.at[pl.ds(0, 26)], as_)

    down.all_sent(0)
    ask.all_sent(0)

    def sent(k, carry):
        gather.all_sent(k)
        return carry

    lax.fori_loop(0, CHUNKS, sent, 0)

    arrived(pieces_in, pr)
    arrived(pieces_in, ps)
    for n in range(15):
        here = here + pieces_in[n].astype(jnp.float32)
    sums[...] = here
    send(sums, sums_in, xs, xr, at.partner())
    gate = mod_mine[:, 128:192]

    def columns_here(value):
        return gate * jnp.where(at.c == 0, value[:, :64], value[:, 64:])

    here = columns_here(here)
    arrived(sums_in, xr)
    there = columns_here(sums_in[...])
    branch = jnp.concatenate([jnp.where(at.c == 0, here, there), jnp.where(at.c == 0, there, here)], axis=0)
    out_ref[...] = (latent_ref[...].astype(jnp.float32) + jnp.transpose(branch)).astype(jnp.bfloat16)
    arrived(sums_in, xs)


def gather_sems(chunks):
    dma = pltpu.SemaphoreType.DMA
    few, many = dma((chunks, 2, 4)), dma((chunks, 2, 4, 4))
    return [few, few, many, many, many, many]


def turn_tables():
    half = ROPE // 2
    inverse = (np.float32(1.0) / np.float32(THETA) ** (np.arange(0, half, 2, dtype=np.float32) / np.float32(half))).astype(
        np.float32
    )

    def table(count, start):
        angle = (np.arange(count, dtype=np.float32)[:, None] * inverse).astype(np.float32)
        cosine, sine = np.cos(angle), np.sin(angle)
        whole_cos = np.zeros((count, 128), np.float32)
        whole_sin = np.zeros((count, 128), np.float32)
        whole_cos[:, start : start + 32] = np.concatenate([cosine, cosine], axis=1)
        whole_sin[:, start : start + 32] = np.concatenate([-sine, sine], axis=1)
        return whole_cos, whole_sin

    return table(6144 // GRID_W, 0) + table(GRID_W, 32)


def per_device(
    latent, context, cond, cond_ctx, w_mod, g_norm, w_dq, w_dkv, w_kr, g_cq, g_ckv, w_uq, w_ukv, ctx_lift, w_out
):
    rows = latent.shape[0]
    vmem = pl.BlockSpec(memory_space=pltpu.VMEM)
    smem = pl.BlockSpec(memory_space=pltpu.SMEM)
    hbm = pl.BlockSpec(memory_space=pltpu.HBM)
    dma = pltpu.SemaphoreType.DMA
    bf16, f32 = jnp.bfloat16, jnp.float32
    return pl.pallas_call(
        main_kernel,
        out_shape=jax.ShapeDtypeStruct((64, rows), bf16),
        in_specs=[vmem] * 11 + [smem] + [vmem] * 4 + [hbm] * 3,
        out_specs=vmem,
        scratch_shapes=[
            pltpu.VMEM((rows, 64), bf16),
            pltpu.VMEM((1, 384), f32),
            pltpu.VMEM((SP - 1, 1, 384), f32),
            pltpu.VMEM((1, 512), f32),
            pltpu.VMEM((32, 1, 512), f32),
            pltpu.VMEM((32, BLOCK, 64), bf16),
            pltpu.VMEM((BLOCK, D), bf16),
            pltpu.VMEM((1, 32, 4, 16, 1152), bf16),
            pltpu.VMEM((1, 32, 4, BLOCK, 128), bf16),
            pltpu.VMEM((4, BLOCK, 128), bf16),
            pltpu.VMEM((BLOCK, 128), bf16),
            pltpu.VMEM((CHUNKS, 4, BLOCK, 128), bf16),
            pltpu.VMEM((NOPE + ROPE, 512), bf16),
            pltpu.VMEM((512, NOPE + DV), bf16),
            pltpu.VMEM((DV, 512), bf16),
            pltpu.VMEM((DV, D), bf16),
            pltpu.VMEM((2, rows, 256), bf16),
            pltpu.VMEM((CHUNKS, 32, 18, BLOCK, 128), bf16),
            pltpu.VMEM((1, rows), f32),
            pltpu.VMEM((1, rows), f32),
            pltpu.VMEM((DV, rows), f32),
            pltpu.VMEM((DV, D), bf16),
            pltpu.VMEM((rows, DV), bf16),
            pltpu.VMEM((rows // 2, DV), bf16),
            pltpu.VMEM((15, rows // 2, 128), bf16),
            pltpu.VMEM((15, rows // 2, 128), bf16),
            pltpu.VMEM((rows // 2, 128), f32),
            pltpu.VMEM((rows // 2, 128), f32),
            dma,
            dma,
            dma,
            dma,
            dma,
            dma,
            dma((CHUNKS,)),
            dma((CHUNKS,)),
            dma((CHUNKS,)),
            dma((CHUNKS,)),
            *gather_sems(1),
            *gather_sems(1),
            *gather_sems(CHUNKS),
            *[dma] * 11,
        ],
        compiler_params=pltpu.CompilerParams(
            collective_id=0, has_side_effects=True, vmem_limit_bytes=56 * 1024 * 1024
        ),
        name="main",
    )(
        latent.T,
        context,
        cond[None, :],
        cond_ctx[None, :],
        jnp.transpose(w_mod, (1, 2, 0)).reshape(192, 128),
        g_norm[None, :],
        w_dq,
        w_dkv,
        w_kr,
        g_cq[None, :],
        g_ckv[None, :],
        ctx_lift.reshape(1, 1),
        *turn_tables(),
        w_uq[:, 0, :].T,
        w_ukv[:, 0, :],
        w_out[0],
    ).T


def solution(mesh):
    return jax.shard_map(
        per_device,
        mesh=mesh,
        in_specs=(
            P("sp", "tp"),
            P("sp", "tp"),
            P("sp"),
            P("sp"),
            P("sp", None, "tp"),
            P("tp"),
            P("tp", None),
            P("tp", None),
            P("tp", None),
            P(),
            P(),
            P(None, "tp", None),
            P(None, "tp", None),
            P("tp"),
            P("tp", None, None),
        ),
        out_specs=P("sp", "tp"),
        check_vma=False,
    )
```

```python
import numpy as np

import jax
import jax.numpy as jnp
from jax import lax
from jax.experimental import pallas as pl
from jax.experimental.pallas import tpu as pltpu

from jax.sharding import PartitionSpec as P

MESH = pl.DeviceIdType.MESH
D = 2048
NOPE = 128
ROPE = 64
DV = 128
GRID_W = 64
EPS = 1e-06
THETA = 10000.0
LOG2E = 1.4426950408889634
SCALE = (NOPE + ROPE) ** (-0.5)

BLOCK = 16
OWNERS = 13
SP = 16
CHUNKS = 4
REL = (0, 1, -1, 2, -2, 3, -3, 4, -4, 5, -5, 6, -6, 7, -7, 8)
FAR_FIRST = tuple(
    sorted(
        [(dy, dx) for dy in range(4) for dx in range(4) if dy or dx],
        key=lambda o: -(min(o[0], 4 - o[0]) + min(o[1], 4 - o[1])),
    )
)


def nn(lhs, rhs):
    return jnp.dot(lhs, rhs, preferred_element_type=jnp.float32)


def nt(lhs, rhs):
    return lax.dot_general(lhs, rhs, (((1,), (1,)), ((), ())), preferred_element_type=jnp.float32)


class Place:
    def __init__(self):
        self.z = lax.axis_index("sp")
        self.t = lax.axis_index("tp")
        self.p = lax.div(self.t, 2)
        self.c = lax.rem(self.t, 2)
        self.y = lax.div(self.p, 4)
        self.x = lax.rem(self.p, 4)
        self.a = self.x * (1 - self.c) + self.y * self.c
        self.b = self.y * (1 - self.c) + self.x * self.c

    def dev(self, a, b):
        p = (4 * b + a) * (1 - self.c) + (4 * a + b) * self.c
        return (self.z, 2 * p + self.c)

    def partner(self):
        return (self.z, 2 * self.p + 1 - self.c)


def around(i, by):
    return lax.rem(i + by + 4, 4)


def exists(a, b):
    return 4 * a + b < OWNERS


def send(src, dst, send_sem, recv_sem, device):
    copy = pltpu.make_async_remote_copy(
        src_ref=src,
        dst_ref=dst,
        send_sem=send_sem,
        recv_sem=recv_sem,
        device_id=device,
        device_id_type=MESH,
    )
    copy.start()


def arrived(ref, sem):
    pltpu.make_async_copy(ref, ref, sem).wait()


class PlaneGather:
    def __init__(self, at, buf, owners, way, sems):
        self.size = buf.shape[2] // 2
        self.at = at
        self.buf = buf
        self.owners = owners
        self.way = way
        self.s1, self.r1, self.s2, self.r2, self.sd, self.rd = sems
        self.offsets = (0, -1, 1, 2)
        self.a, self.b = (at.a, at.b) if way == 0 else (at.b, at.a)

    def natural(self, a, b):
        return (a, b) if self.way == 0 else (b, a)

    def dev(self, a, b):
        return self.at.dev(*self.natural(a, b))

    def exists(self, a, b):
        a, b = self.natural(a, b)
        return 4 * a + b < self.owners

    def block(self, k, a, b, core=None):
        a, b = self.natural(a, b)
        core = self.at.c if core is None else core
        return self.buf.at[k, core * 16 + 4 * a + b, pl.ds(self.size * self.way, self.size)]

    def across(self, k, a, b, j, m):
        block = self.block(k, a, b)
        send(block, block, self.sd.at[k, self.way, j, m], self.rd.at[k, self.way, j, m], self.at.partner())

    def first_start(self, k):
        @pl.when(self.exists(self.a, self.b))
        def _():
            own = self.block(k, self.a, self.b)
            for role, by in ((0, 1), (1, -1)):
                send(own, own, self.s1.at[k, self.way, role], self.r1.at[k, self.way, role], self.dev(around(self.a, by), self.b))

    def first_forward(self, k):
        for role, by in ((0, -1), (1, 1)):
            a = around(self.a, by)

            @pl.when(self.exists(a, self.b))
            def _():
                block = self.block(k, a, self.b)
                arrived(block, self.r1.at[k, self.way, role])
                if role == self.way:
                    send(block, block, self.s1.at[k, self.way, 2], self.r1.at[k, self.way, 2], self.dev(around(self.a, -by), self.b))

    def first_end(self, k):
        a = around(self.a, 2)

        @pl.when(self.exists(a, self.b))
        def _():
            arrived(self.block(k, a, self.b), self.r1.at[k, self.way, 2])

    def second_start(self, k, j):
        a = around(self.a, self.offsets[j])

        @pl.when(self.exists(a, self.b))
        def _():
            own = self.block(k, a, self.b)
            for role, by in ((0, 1), (1, -1)):
                send(
                    own, own, self.s2.at[k, self.way, j, role], self.r2.at[k, self.way, j, role], self.dev(self.a, around(self.b, by))
                )
            self.across(k, a, self.b, j, 0)

    def second_forward(self, k, j):
        a = around(self.a, self.offsets[j])
        for role, by in ((0, -1), (1, 1)):
            b = around(self.b, by)

            @pl.when(self.exists(a, b))
            def _():
                block = self.block(k, a, b)
                arrived(block, self.r2.at[k, self.way, j, role])
                if role == j % 2:
                    send(
                        block,
                        block,
                        self.s2.at[k, self.way, j, 2],
                        self.r2.at[k, self.way, j, 2],
                        self.dev(self.a, around(self.b, -by)),
                    )
                self.across(k, a, b, j, 1 + role)

    def second_end(self, k, j):
        a = around(self.a, self.offsets[j])
        b = around(self.b, 2)

        @pl.when(self.exists(a, b))
        def _():
            arrived(self.block(k, a, b), self.r2.at[k, self.way, j, 2])
            self.across(k, a, b, j, 3)

    def other_core(self, k):
        for j in range(4):
            a = around(self.b, self.offsets[j])
            for m in range(4):
                b = around(self.a, self.offsets[m])

                @pl.when(self.exists(a, b))
                def _():
                    arrived(self.block(k, a, b, 1 - self.at.c), self.rd.at[k, self.way, j, m])

    def all_sent(self, k):
        own = self.block(k, 0, 0)

        @pl.when(self.exists(self.a, self.b))
        def _():
            arrived(own, self.s1.at[k, self.way, 0])
            arrived(own, self.s1.at[k, self.way, 1])

        @pl.when(self.exists(around(self.a, 1 if self.way else -1), self.b))
        def _():
            arrived(own, self.s1.at[k, self.way, 2])

        for j in range(4):
            a = around(self.a, self.offsets[j])

            @pl.when(self.exists(a, self.b))
            def _():
                arrived(own, self.s2.at[k, self.way, j, 0])
                arrived(own, self.s2.at[k, self.way, j, 1])
                arrived(own, self.sd.at[k, self.way, j, 0])

            for role, by in ((0, -1), (1, 1)):

                @pl.when(self.exists(a, around(self.b, by)))
                def _():
                    if role == j % 2:
                        arrived(own, self.s2.at[k, self.way, j, 2])
                    arrived(own, self.sd.at[k, self.way, j, 1 + role])

            @pl.when(self.exists(a, around(self.b, 2)))
            def _():
                arrived(own, self.sd.at[k, self.way, j, 3])


class BothWays:
    def __init__(self, at, buf, owners, sems):
        self.ways = [PlaneGather(at, buf, owners, way, sems) for way in range(2)]

    def __getattr__(self, name):
        def call(*args):
            for way in self.ways:
                getattr(way, name)(*args)

        return call


def swapped(values):
    lane = lax.broadcasted_iota(jnp.int32, values.shape, 1)
    return jnp.where(lax.rem(lane, 32) < 16, pltpu.roll(values, 112, 1), pltpu.roll(values, 16, 1))


def low_norm(values, gain):
    scale = lax.rsqrt(jnp.mean(values * values, axis=-1, keepdims=True) + EPS)
    return (values * scale * gain).astype(jnp.bfloat16)


def main_kernel(
    latent_ref,
    context_ref,
    cond_ref,
    cond_ctx_ref,
    w_mod_ref,
    g_norm_ref,
    w_dq_ref,
    w_dkv_ref,
    w_kr_ref,
    g_cq_ref,
    g_ckv_ref,
    lift_ref,
    row_cos_ref,
    row_sin_ref,
    col_cos_ref,
    col_sin_ref,
    w_uq_hbm,
    w_ukv_hbm,
    w_out_hbm,
    out_ref,
    latent,
    mod_part,
    mod_in,
    mod_mine,
    mod_all,
    x_all,
    h_all,
    w_down,
    compressed,
    item,
    turned,
    turned_in,
    w_uq,
    w_up,
    w_uvt,
    w_out,
    query,
    keys,
    peak,
    total,
    accum,
    w_other,
    heads,
    heads_in,
    pieces,
    pieces_in,
    sums,
    sums_in,
    ms,
    mr,
    as_,
    ar,
    vs,
    vr,
    zs,
    zr,
    ts,
    tr,
    *rest,
):
    down_sems, cq_sems, key_sems = rest[0:6], rest[6:12], rest[12:18]
    ws, wr, hs, hr, ps, pr, xs, xr, l1, l2, l3 = rest[18:]
    at = Place()
    owner = exists(at.a, at.b)
    own_slot = at.c * 16 + 4 * at.a + at.b
    own_item = jnp.minimum(at.c * OWNERS + 4 * at.a + at.b, 25)
    in_context = own_item >= 24

    barrier = pltpu.get_barrier_semaphore()

    def greet_z(i, carry):
        pl.semaphore_signal(barrier, inc=1, device_id=(lax.rem(at.z + i, SP), at.t), device_id_type=MESH)
        return carry

    def greet_plane(i, carry):
        pl.semaphore_signal(barrier, inc=1, device_id=(at.z, lax.rem(at.t + i, 32)), device_id_type=MESH)
        return carry

    lax.fori_loop(1, SP, greet_z, 0)
    lax.fori_loop(1, 32, greet_plane, 0)

    loads = [
        pltpu.make_async_copy(w_uq_hbm, w_uq, l1),
        pltpu.make_async_copy(w_ukv_hbm, w_up, l2),
        pltpu.make_async_copy(w_out_hbm, w_out, l3),
    ]
    for load in loads:
        load.start()

    for n in range(4):
        rows = pl.ds(n * 16, 16)
        w_down[0, own_slot, n, :, 0:512] = w_dq_ref[rows, :]
        w_down[0, own_slot, n, :, 512:1024] = w_dkv_ref[rows, :]
        w_down[0, own_slot, n, :, 1024:1152] = jnp.concatenate(
            [w_kr_ref[rows, :], jnp.zeros((16, 64), jnp.bfloat16)], axis=1
        )
    latent[...] = jnp.transpose(latent_ref[...].astype(jnp.float32)).astype(jnp.bfloat16)
    signal = jnp.concatenate([cond_ref[...], cond_ctx_ref[...], jnp.zeros((6, 128), jnp.bfloat16)], axis=0)
    signal = jax.nn.silu(signal.astype(jnp.float32)).astype(jnp.bfloat16)
    partial_mod = nt(signal, w_mod_ref[...])
    mod_part[:, 0:192] = partial_mod[0:1]
    mod_part[:, 192:384] = partial_mod[1:2]
    mod_mine[...] = jnp.zeros(mod_mine.shape, jnp.float32)
    peak[...] = jnp.full(peak.shape, -1e30, jnp.float32)
    total[...] = jnp.zeros(total.shape, jnp.float32)
    accum[...] = jnp.zeros(accum.shape, jnp.float32)

    pl.semaphore_wait(barrier, 46)

    for n in range(1, SP):
        send(mod_part, mod_in.at[n - 1], ms, mr, (lax.rem(at.z - REL[n] + SP, SP), at.t))

    down = BothWays(at, w_down, 16, down_sems)
    down.first_start(0)
    down.second_start(0, 0)

    down.first_forward(0)
    down.second_start(0, 1)
    down.second_start(0, 2)
    loads[1].wait()
    w_uvt[...] = jnp.transpose(w_up[:, NOPE:].astype(jnp.float32)).astype(jnp.bfloat16)
    down.first_end(0)
    down.second_start(0, 3)

    def give(i, source):
        c = lax.div(i, OWNERS)
        l = i - c * OWNERS
        a, b = lax.div(l, 4), lax.rem(l, 4)
        t = 2 * ((4 * b + a) * (1 - c) + (4 * a + b) * c) + c

        @pl.when(t != at.t)
        def _():
            send(source, x_all.at[own_slot], as_, ar, (at.z, t))

        @pl.when(t == at.t)
        def _():
            x_all[own_slot] = source[...]

    def give_latent(i, carry):
        give(i, latent.at[pl.ds(pl.multiple_of(i * BLOCK, BLOCK), BLOCK)])
        return carry

    lax.fori_loop(0, 24, give_latent, 0)
    for i in (24, 25):
        give(jnp.int32(i), context_ref.at[pl.ds((i - 24) * BLOCK, BLOCK)])


    arrived(mod_in, mr)
    mod = mod_part[...]
    for n in range(SP - 1):
        mod = mod + mod_in[n]
    mod_mine[:, 0:384] = mod
    mod_mine[:, 384:448] = g_norm_ref[...]
    mod_all[own_slot] = mod_mine[...]

    def tell(i, carry):
        send(mod_mine, mod_all.at[own_slot], vs, vr, (at.z, lax.rem(at.t + i, 32)))
        return carry

    lax.fori_loop(1, 32, tell, 0)

    for j in range(4):
        down.second_forward(0, j)

    @pl.when(owner)
    def _():
        arrived(x_all.at[pl.ds(0, 31)], ar)

    x = x_all[...].astype(jnp.float32)
    squares = jnp.sum(jnp.sum(x * x, axis=0), axis=1, keepdims=True)
    norm = lax.rsqrt(squares / D + EPS)
    for j in range(4):
        down.second_end(0, j)
    loads[2].wait()
    send(w_out, w_other, ws, wr, at.partner())
    arrived(mod_all.at[pl.ds(0, 31)], vr)
    for s in range(0, 32, 2):
        pair = []
        for slot in (s, s + 1):
            m = mod_all[slot]
            shift = jnp.where(in_context, m[:, 192:256], m[:, 0:64])
            scale = jnp.where(in_context, m[:, 256:320], m[:, 64:128])
            pair.append((x[slot] * norm * m[:, 384:448] * (1.0 + scale) + shift).astype(jnp.bfloat16))
        h_all[:, s * 64 : s * 64 + 128] = jnp.concatenate(pair, axis=1)
    down.other_core(0)
    low = nn(h_all[...], w_down[0].reshape(D, 1152))

    first_row = at.z * 6
    item_row = first_row + lax.div(jnp.minimum(own_item, 23), 4)
    item_col = pl.ds(pl.multiple_of(lax.rem(own_item, 4) * BLOCK, BLOCK), BLOCK)
    item_cos = jnp.where(in_context, 1.0, row_cos_ref[pl.ds(item_row, 1), :] + col_cos_ref[item_col, :])
    item_sin = jnp.where(in_context, 0.0, row_sin_ref[pl.ds(item_row, 1), :] + col_sin_ref[item_col, :])
    rotary = low[:, 1024:1152]
    rotary = rotary * item_cos + swapped(rotary) * item_sin
    ckv_own = low_norm(low[:, 512:1024], g_ckv_ref[...])
    for n in range(4):
        item[n] = ckv_own[:, 128 * n : 128 * n + 128]
    turned[...] = (rotary + pltpu.roll(rotary, 64, 1)).astype(jnp.bfloat16)
    cq = low_norm(low[:, 0:512], g_cq_ref[...])
    for n in range(4):
        compressed[0, own_slot, n] = cq[:, 128 * n : 128 * n + 128]

    @pl.when(owner)
    def _():
        keys[0, own_slot, 0:4] = item[...]
        turned_in[0, 0] = turned[...]
        for n in range(1, SP):
            k, i = divmod(n, 4)
            there = (lax.rem(at.z - REL[n] + SP, SP), at.t)
            send(item, keys.at[k, own_slot, pl.ds(9 * (i // 2) + 4 * (i % 2), 4)], zs.at[k], zr.at[k], there)
            send(turned, turned_in.at[k, i], ts.at[k], tr.at[k], there)

    ask = BothWays(at, compressed, OWNERS, cq_sems)
    gather = BothWays(at, keys, OWNERS, key_sems)
    ask.first_start(0)
    ask.second_start(0, 0)

    def join_turned(k):
        for way in range(2):
            first = turned_in[k, 2 * way].astype(jnp.float32)
            second = turned_in[k, 2 * way + 1].astype(jnp.float32)
            lane = lax.broadcasted_iota(jnp.int32, first.shape, 1)
            keys[k, own_slot, 9 * way + 8] = jnp.where(lane < 64, first, second).astype(jnp.bfloat16)

    def chunk_here(k):
        @pl.when(owner)
        def _():
            arrived(keys.at[k, own_slot, pl.ds(0, 16)], zr.at[k])
            arrived(turned_in.at[k], tr.at[k])
            join_turned(k)

    lift = lift_ref[0, 0] * LOG2E

    def attend(k, g):
        slots = pl.ds(g * 16, OWNERS)
        count = OWNERS * BLOCK
        ckv = jnp.concatenate(
            [
                jnp.concatenate([keys[k, slots, 9 * w + 4 * i + n].reshape(count, 128) for n in range(4)], axis=1)
                for w in range(2)
                for i in range(2)
            ],
            axis=0,
        )
        key = nn(ckv, w_up[:, :NOPE]).astype(jnp.bfloat16)
        value = nt(w_uvt[...], ckv).astype(jnp.bfloat16)
        extra = jnp.where(g == 1, lift, 0.0)
        scores = []
        for w in range(2):
            rotary_key = keys[k, slots, 9 * w + 8].reshape(count, 128)
            for i in range(2):
                first = (2 * w + i) * count
                both = jnp.concatenate([key[first : first + count], rotary_key], axis=1)
                part = nt(both, query[i]) * (SCALE * LOG2E)
                scores += [part[: 11 * BLOCK], part[11 * BLOCK :] + extra]
        score = jnp.concatenate(scores, axis=0)
        fresh = jnp.maximum(peak[...], jnp.max(score, axis=0, keepdims=True))
        probs = jnp.exp2(score - fresh)
        fade = jnp.exp2(peak[...] - fresh)
        peak[...] = fresh
        total[...] = total[...] * fade + jnp.sum(probs, axis=0, keepdims=True)
        accum[...] = accum[...] * fade + nn(value, probs.astype(jnp.bfloat16))

    @pl.when(owner)
    def _():
        arrived(keys.at[0, own_slot, pl.ds(0, 12)], zr.at[0])
        arrived(turned_in.at[0, pl.ds(1, 3)], tr.at[0])
        join_turned(0)

    gather.first_start(0)
    gather.second_start(0, 0)
    ask.first_forward(0)
    ask.second_start(0, 1)
    ask.second_start(0, 2)
    gather.first_forward(0)
    gather.second_start(0, 1)
    gather.second_start(0, 2)
    ask.first_end(0)
    ask.second_start(0, 3)
    gather.first_end(0)
    gather.second_start(0, 3)
    chunk_here(1)
    gather.first_start(1)
    for j in range(4):
        ask.second_forward(0, j)
    for j in range(4):
        ask.second_end(0, j)

    def make_query():
        loads[0].wait()
        ask.other_core(0)
        cq = jnp.concatenate(
            [
                jnp.concatenate([compressed[0, pl.ds(16 * c, 13 - 2 * c), n].reshape(-1, 128) for n in range(4)], axis=1)
                for c in range(2)
            ],
            axis=0,
        )
        plain = nt(cq, w_uq[0:NOPE, :]).astype(jnp.bfloat16)
        query[0, :, 0:NOPE] = plain
        query[1, :, 0:NOPE] = plain
        turn = nt(cq, w_uq[NOPE:, :])
        turn = jnp.concatenate([turn, jnp.zeros_like(turn)], axis=1)
        for r in range(6):
            values = turn[64 * r : 64 * r + 64]
            cosine = row_cos_ref[pl.ds(first_row + r, 1), :] + col_cos_ref[...]
            sine = row_sin_ref[pl.ds(first_row + r, 1), :] + col_sin_ref[...]
            values = values * cosine + swapped(values) * sine
            query[0, 64 * r : 64 * r + 64, NOPE:] = values.astype(jnp.bfloat16)
            query[1, 64 * r : 64 * r + 64, NOPE:] = pltpu.roll(values, 64, 1).astype(jnp.bfloat16)

    def step(k, carry):
        @pl.when(k < CHUNKS)
        def _():
            gather.second_forward(k, 0)
            gather.second_forward(k, 1)

        @pl.when(k == 0)
        def _():
            make_query()

        @pl.when(k > 0)
        def _():
            attend(k - 1, at.c)

        @pl.when(k < CHUNKS - 1)
        def _():
            gather.first_forward(k + 1)
            gather.second_start(k + 1, 0)
            gather.second_start(k + 1, 1)
            gather.second_start(k + 1, 2)

        @pl.when(k < CHUNKS)
        def _():
            gather.second_forward(k, 2)
            gather.second_forward(k, 3)

        @pl.when(k < CHUNKS - 1)
        def _():
            gather.first_end(k + 1)
            gather.second_start(k + 1, 3)

        @pl.when(k < CHUNKS - 2)
        def _():
            chunk_here(k + 2)
            gather.first_start(k + 2)

        @pl.when(k > 0)
        def _():
            gather.other_core(k - 1)
            attend(k - 1, 1 - at.c)

        @pl.when(k < CHUNKS)
        def _():
            for j in range(4):
                gather.second_end(k, j)

        return carry

    lax.fori_loop(0, CHUNKS + 1, step, 0)

    rows = heads_in.shape[0]
    heads[...] = jnp.transpose(accum[...] / total[...]).astype(jnp.bfloat16)
    theirs = heads.at[pl.ds((1 - at.c) * rows, rows)]
    send(theirs, heads_in, hs, hr, at.partner())
    mine = heads[pl.ds(at.c * rows, rows), :]

    def columns_of(p):
        return pl.ds(pl.multiple_of(p * 128, 128), 128)

    targets = [4 * around(at.y, dy) + around(at.x, dx) for dy, dx in FAR_FIRST]
    early = [nn(mine, w_out[:, columns_of(p)]) for p in targets[:6]]
    arrived(w_other, wr)
    arrived(heads_in, hr)
    other = heads_in[...]

    def product(p, own=None):
        own = nn(mine, w_out[:, columns_of(p)]) if own is None else own
        return own + nn(other, w_other[:, columns_of(p)])

    for n, p in enumerate(targets):
        pieces[n] = product(p, early[n] if n < len(early) else None).astype(jnp.bfloat16)
        send(pieces.at[n], pieces_in.at[n], ps, pr, (at.z, 2 * p + at.c))
    here = product(at.p)
    arrived(mod_in, ms)
    arrived(mod_all.at[pl.ds(0, 31)], vs)
    arrived(w_other, ws)
    arrived(heads_in, hs)

    @pl.when(owner)
    def _():
        arrived(x_all.at[pl.ds(0, 25)], as_)
        arrived(keys.at[0, 0, pl.ds(0, 12)], zs.at[0])
        arrived(turned_in.at[0, pl.ds(1, 3)], ts.at[0])
        for k in range(1, CHUNKS):
            arrived(keys.at[k, 0, pl.ds(0, 16)], zs.at[k])
            arrived(turned_in.at[k], ts.at[k])

    @pl.when(jnp.logical_not(owner))
    def _():
        arrived(x_all.at[pl.ds(0, 26)], as_)

    down.all_sent(0)
    ask.all_sent(0)

    def sent(k, carry):
        gather.all_sent(k)
        return carry

    lax.fori_loop(0, CHUNKS, sent, 0)

    arrived(pieces_in, pr)
    arrived(pieces_in, ps)
    for n in range(15):
        here = here + pieces_in[n].astype(jnp.float32)
    sums[...] = here
    send(sums, sums_in, xs, xr, at.partner())
    gate = mod_mine[:, 128:192]

    def columns_here(value):
        return gate * jnp.where(at.c == 0, value[:, :64], value[:, 64:])

    here = columns_here(here)
    arrived(sums_in, xr)
    there = columns_here(sums_in[...])
    branch = jnp.concatenate([jnp.where(at.c == 0, here, there), jnp.where(at.c == 0, there, here)], axis=0)
    out_ref[...] = (latent_ref[...].astype(jnp.float32) + jnp.transpose(branch)).astype(jnp.bfloat16)
    arrived(sums_in, xs)


def gather_sems(chunks):
    dma = pltpu.SemaphoreType.DMA
    few, many = dma((chunks, 2, 4)), dma((chunks, 2, 4, 4))
    return [few, few, many, many, many, many]


def turn_tables():
    half = ROPE // 2
    inverse = (np.float32(1.0) / np.float32(THETA) ** (np.arange(0, half, 2, dtype=np.float32) / np.float32(half))).astype(
        np.float32
    )

    def table(count, start):
        angle = (np.arange(count, dtype=np.float32)[:, None] * inverse).astype(np.float32)
        cosine, sine = np.cos(angle), np.sin(angle)
        whole_cos = np.zeros((count, 128), np.float32)
        whole_sin = np.zeros((count, 128), np.float32)
        whole_cos[:, start : start + 32] = np.concatenate([cosine, cosine], axis=1)
        whole_sin[:, start : start + 32] = np.concatenate([-sine, sine], axis=1)
        return whole_cos, whole_sin

    return table(6144 // GRID_W, 0) + table(GRID_W, 32)


def per_device(
    latent, context, cond, cond_ctx, w_mod, g_norm, w_dq, w_dkv, w_kr, g_cq, g_ckv, w_uq, w_ukv, ctx_lift, w_out
):
    rows = latent.shape[0]
    vmem = pl.BlockSpec(memory_space=pltpu.VMEM)
    smem = pl.BlockSpec(memory_space=pltpu.SMEM)
    hbm = pl.BlockSpec(memory_space=pltpu.HBM)
    dma = pltpu.SemaphoreType.DMA
    bf16, f32 = jnp.bfloat16, jnp.float32
    return pl.pallas_call(
        main_kernel,
        out_shape=jax.ShapeDtypeStruct((64, rows), bf16),
        in_specs=[vmem] * 11 + [smem] + [vmem] * 4 + [hbm] * 3,
        out_specs=vmem,
        scratch_shapes=[
            pltpu.VMEM((rows, 64), bf16),
            pltpu.VMEM((1, 384), f32),
            pltpu.VMEM((SP - 1, 1, 384), f32),
            pltpu.VMEM((1, 512), f32),
            pltpu.VMEM((32, 1, 512), f32),
            pltpu.VMEM((32, BLOCK, 64), bf16),
            pltpu.VMEM((BLOCK, D), bf16),
            pltpu.VMEM((1, 32, 4, 16, 1152), bf16),
            pltpu.VMEM((1, 32, 4, BLOCK, 128), bf16),
            pltpu.VMEM((4, BLOCK, 128), bf16),
            pltpu.VMEM((BLOCK, 128), bf16),
            pltpu.VMEM((CHUNKS, 4, BLOCK, 128), bf16),
            pltpu.VMEM((NOPE + ROPE, 512), bf16),
            pltpu.VMEM((512, NOPE + DV), bf16),
            pltpu.VMEM((DV, 512), bf16),
            pltpu.VMEM((DV, D), bf16),
            pltpu.VMEM((2, rows, 256), bf16),
            pltpu.VMEM((CHUNKS, 32, 18, BLOCK, 128), bf16),
            pltpu.VMEM((1, rows), f32),
            pltpu.VMEM((1, rows), f32),
            pltpu.VMEM((DV, rows), f32),
            pltpu.VMEM((DV, D), bf16),
            pltpu.VMEM((rows, DV), bf16),
            pltpu.VMEM((rows // 2, DV), bf16),
            pltpu.VMEM((15, rows // 2, 128), bf16),
            pltpu.VMEM((15, rows // 2, 128), bf16),
            pltpu.VMEM((rows // 2, 128), f32),
            pltpu.VMEM((rows // 2, 128), f32),
            dma,
            dma,
            dma,
            dma,
            dma,
            dma,
            dma((CHUNKS,)),
            dma((CHUNKS,)),
            dma((CHUNKS,)),
            dma((CHUNKS,)),
            *gather_sems(1),
            *gather_sems(1),
            *gather_sems(CHUNKS),
            *[dma] * 11,
        ],
        compiler_params=pltpu.CompilerParams(
            collective_id=0, has_side_effects=True, vmem_limit_bytes=56 * 1024 * 1024
        ),
        name="main",
    )(
        latent.T,
        context,
        cond[None, :],
        cond_ctx[None, :],
        jnp.transpose(w_mod, (1, 2, 0)).reshape(192, 128),
        g_norm[None, :],
        w_dq,
        w_dkv,
        w_kr,
        g_cq[None, :],
        g_ckv[None, :],
        ctx_lift.reshape(1, 1),
        *turn_tables(),
        w_uq[:, 0, :].T,
        w_ukv[:, 0, :],
        w_out[0],
    ).T


def solution(mesh):
    return jax.shard_map(
        per_device,
        mesh=mesh,
        in_specs=(
            P("sp", "tp"),
            P("sp", "tp"),
            P("sp"),
            P("sp"),
            P("sp", None, "tp"),
            P("tp"),
            P("tp", None),
            P("tp", None),
            P("tp", None),
            P(),
            P(),
            P(None, "tp", None),
            P(None, "tp", None),
            P("tp"),
            P("tp", None, None),
        ),
        out_specs=P("sp", "tp"),
        check_vma=False,
    )
```
